32 devices in a mesh: ep: 4 (over z), tp: 8 (over y, x, core).
Axes of the slice: x: 2, y: 2, z: 4, core: 2. Of those that a mesh axis runs over, the one named last changes fastest.
Arguments:
- tokens: bfloat16 [4096, 2048], P(('ep', 'tp')), may hold values from -40 to 40
- norm_gain: float32 [2048], replicated, may hold values from 0.1 to 1.9
- routes: int32 [4096, 2], P(('ep', 'tp')), may hold values from 0 to 7, all different within a row; in each aligned block of 128 rows (0 to 127, 128 to 255, ...) at most 64 rows name the same one
- gates: float32 [4096, 2], P(('ep', 'tp')), may hold values from 0.25 to 2
- expert_gate: bfloat16 [8, 2048, 512], P('tp'), may hold values from -0.125 to 0.125
- expert_up: bfloat16 [8, 2048, 512], P('tp'), may hold values from -0.125 to 0.125
- expert_down: bfloat16 [8, 512, 2048], P('tp'), may hold values from -0.25 to 0.25
- shared_gate: bfloat16 [2048, 256], replicated, may hold values from -0.125 to 0.125
- shared_up: bfloat16 [2048, 256], replicated, may hold values from -0.125 to 0.125
- shared_down: bfloat16 [256, 2048], replicated, may hold values from -0.375 to 0.375
Outputs:
- mixed: bfloat16 [4096, 2048], P(('ep', 'tp'))
- load: float32 [8], replicated
The draws below stay inside these ranges and needn't reach their ends.
Inputs may be any that keep to these rules, and one draw needn't show every extreme that they name: `routes`: each row names 2 different experts. Among the rows of one device no expert is named by more than 64 rows, and in every draw some expert is named by exactly 64 rows of some device.
All inputs are finite; a program needn't handle non-finite values.
Results may differ from the reference program's by a relative error of at most 0.002.
The reference program's roundings to bfloat16 on the way count: a program that leaves them out, or rounds other values in their place, can miss the bound.
Values may be sent and summed in bfloat16 or wider, within the bound.
A program may use at most 64 MiB of HBM per device.

```python
import math
import jax
import jax.numpy as jnp
import numpy as np
from jax import lax

D = 2048
EXPERT_UNITS = 512
SHARED = 256
TOPK = 2
TOK_DEV = 128
EXPERTS = 8
CAP = 64
TOKENS = 4096


def draw_tokens(key, part):
    key_values, key_column, key_row = jax.random.split(key, 3)
    column_scale = jnp.exp(jax.random.uniform(key_column, (D,), jnp.float32, jnp.log(0.5), jnp.log(5.0)))
    row_scale = jnp.exp(jax.random.uniform(key_row, (TOKENS, 1), jnp.float32, jnp.log(0.5), jnp.log(2.0)))
    base_values = jnp.clip(jax.random.normal(key_values, (TOKENS, D), jnp.float32), -4.0, 4.0)
    return (base_values * column_scale * row_scale).astype(jnp.bfloat16)


def level_of(stream_key, shape, pieces, low, high):
    level, own = 1.0, jax.random.fold_in(stream_key, 6)
    for axis_at, parts in pieces:
        heights = jnp.exp(jax.random.uniform(jax.random.fold_in(own, axis_at), (parts,), jnp.float32, low / len(pieces), high / len(pieces)))
        level = level * jnp.repeat(heights, shape[axis_at] // parts).reshape([-1 if axis == axis_at else 1 for axis in range(len(shape))])
    return level


def routed_block(own_key, own, number, rows, number_of, top, bound, skew):
    ranking = jax.random.permutation(own_key, number_of)
    crowded, ordinary = load_shares(number_of, rows * top, bound, skew, True), load_shares(number_of, rows * top, bound, skew, False)
    places = jnp.arange(number_of)

    def named(lengths, rotation):
        used = int((lengths > 0).sum())
        fixed = max(1, used // 4)
        passed = fixed + (places - fixed + rotation * (used - fixed)) % max(1, number_of - fixed)
        return jnp.zeros((number_of,), jnp.int32).at[ranking[jnp.where(places < fixed, places, passed)]].set(jnp.asarray(lengths, jnp.int32))

    lengths = jnp.where(number % 4 == 0, named(crowded, number // 4), named(ordinary, number - number // 4 - 1))
    mixed = jax.random.permutation(jax.random.fold_in(own, 3), number_of)
    donor, sink = mixed[0:number_of // 2 * 2:2], mixed[1:number_of // 2 * 2:2]
    slack = jnp.minimum(lengths[donor] - 1, bound - lengths[sink]) // 2
    slack = jnp.where((donor == ranking[0]) | (sink == ranking[0]) | (lengths[sink] == 0), 0, jnp.maximum(slack, 0))
    passed = jax.random.randint(jax.random.fold_in(own, 4), (number_of // 2,), 0, 1 << 20) % (slack + 1)
    lengths = lengths.at[donor].add(-passed).at[sink].add(passed)
    items = jnp.searchsorted(jnp.cumsum(lengths), jnp.arange(rows * top), side="right").astype(jnp.int32)
    table = items.reshape(top, rows).T
    table = table[jax.random.permutation(jax.random.fold_in(own, 1), rows)]
    rotation = jax.random.randint(jax.random.fold_in(own, 2), (rows, 1), 0, top)
    return jnp.take_along_axis(table, (jnp.arange(top)[None, :] + rotation) % top, axis=1)


def load_shares(amount, total, reach, lean, full):
    portions = [(1 << 20) // math.isqrt(grade ** lean) + 1 for grade in range(1, amount + 1)]
    largest = reach if full else min(reach, max(-(-total // amount), total * portions[0] // sum(portions)))
    least = 1 if total - largest >= amount - 1 else 0
    given, rest = [largest] + [least] * (amount - 1), total - largest - least * (amount - 1)
    while rest > 0:
        candidates = [i for i in range(1, amount) if given[i] < largest] or [i for i in range(1, amount) if given[i] < reach]
        whole, budget = sum([portions[i] for i in candidates]), rest
        for i in candidates:
            more = min(reach - given[i], max(1, budget * portions[i] // whole), rest)
            given[i] = given[i] + more
            rest = rest - more
    return np.array(given)


def scatter_about(key, extent, deviation, reach, cuts=(), kind=jnp.bfloat16):
    gain = level_of(key, extent, cuts, -0.22, 0.18) if cuts else 1.0
    drawn = jax.random.normal(key, extent, jnp.float32) * deviation * gain
    return jnp.minimum(jnp.maximum(drawn, -reach), reach).astype(kind)


def setup_inputs(seed: int = 0) -> dict:
    streams_of = jax.random.split(jax.random.key(seed), 11)
    tokens = draw_tokens(jax.random.fold_in(streams_of[10], 71), 0)
    norm_gain = jnp.clip(1.0 + 0.18 * jax.random.normal(streams_of[1], (D,), jnp.float32), 0.1, 1.9)
    routes_keys = jax.random.split(jax.random.fold_in(streams_of[2], 1), TOKENS // TOK_DEV)
    routes_turns = jax.random.permutation(jax.random.fold_in(streams_of[2], 3), TOKENS // TOK_DEV)
    routes = jax.vmap(lambda own, number: routed_block(jax.random.fold_in(streams_of[2], 2), own, number, TOK_DEV, EXPERTS, TOPK, CAP, 2))(routes_keys, routes_turns).reshape((TOKENS, TOPK))
    gates = jnp.clip(0.25 + 1.75 * jax.random.uniform(streams_of[3], (TOKENS, TOPK), jnp.float32) ** level_of(streams_of[3], (TOKENS, TOPK), ((0, 32),), -0.2, 0.2), 0.25, 2.0)
    expert_gate = scatter_about(streams_of[4], (EXPERTS, D, EXPERT_UNITS), D ** -0.5, 0.125, ((0, 8),))
    expert_up = scatter_about(streams_of[5], (EXPERTS, D, EXPERT_UNITS), D ** -0.5, 0.125, ((0, 8),))
    expert_down = scatter_about(streams_of[6], (EXPERTS, EXPERT_UNITS, D), EXPERT_UNITS ** -0.5, 0.25, ((0, 8),))
    shared_gate = scatter_about(streams_of[7], (D, SHARED), D ** -0.5, 0.125)
    shared_up = scatter_about(streams_of[8], (D, SHARED), D ** -0.5, 0.125)
    shared_down = scatter_about(streams_of[9], (SHARED, D), SHARED ** -0.5, 0.375)
    return dict(tokens=tokens, norm_gain=norm_gain, routes=routes, gates=gates, expert_gate=expert_gate, expert_up=expert_up, expert_down=expert_down, shared_gate=shared_gate, shared_up=shared_up, shared_down=shared_down)


block_rows = 512

def layer_normed(token_block, norm_gain):
    values = token_block.astype(jnp.float32)
    center = lax.optimization_barrier(jnp.mean(values, axis=-1, keepdims=True))
    spread = lax.optimization_barrier(jnp.mean(jnp.square(values - center), axis=-1, keepdims=True))
    return ((values - center) * lax.rsqrt(spread + 1e-05) * norm_gain).astype(jnp.bfloat16)

def gated_mlp(row_block, w_gate, w_up, w_down):
    gate_part = jnp.dot(row_block, w_gate, preferred_element_type=jnp.float32)
    up_part = jnp.dot(row_block, w_up, preferred_element_type=jnp.float32)
    hidden = (jax.nn.silu(gate_part) * up_part).astype(jnp.bfloat16)
    return jnp.dot(hidden, w_down, preferred_element_type=jnp.float32)

def reference(tokens, norm_gain, routes, gates, expert_gate, expert_up, expert_down, shared_gate, shared_up, shared_down):
    normed = layer_normed(tokens, norm_gain)
    count_rows, feature_count = normed.shape
    copy_count = count_rows * TOPK
    flat_expert = routes.reshape(-1).astype(jnp.int32)
    flat_token = jnp.repeat(jnp.arange(count_rows, dtype=jnp.int32), TOPK)
    sort_order = jnp.argsort(flat_expert, stable=True).astype(jnp.int32)
    sorted_expert = flat_expert[sort_order]
    counts = lax.optimization_barrier(jnp.sum((flat_expert[:, None] == jnp.arange(EXPERTS, dtype=jnp.int32)[None, :]).astype(jnp.int32), axis=0))
    padded = (counts + block_rows - 1) // block_rows * block_rows
    starts = jnp.cumsum(counts) - counts
    block_ends = jnp.cumsum(padded)
    padded_starts = block_ends - padded
    destination = (padded_starts[sorted_expert] + jnp.arange(copy_count, dtype=jnp.int32) - starts[sorted_expert]).astype(jnp.int32)
    block_count = -(-copy_count // block_rows) + EXPERTS
    slot_token = jnp.full((block_count * block_rows,), count_rows, jnp.int32).at[destination].set(flat_token[sort_order])
    block_expert = jnp.clip(jnp.searchsorted(block_ends, jnp.arange(block_count, dtype=jnp.int32) * block_rows, side='right'), 0, EXPERTS - 1).astype(jnp.int32)
    padded_rows = jnp.concatenate([normed, jnp.zeros((1, feature_count), normed.dtype)], axis=0)

    def run_block(block_item):
        slot_tokens, expert = block_item
        row_block = padded_rows[slot_tokens]
        return gated_mlp(row_block, expert_gate[expert], expert_up[expert], expert_down[expert]).astype(jnp.bfloat16)
    slot_out = lax.map(run_block, (slot_token.reshape(block_count, block_rows), block_expert))
    slot_out = slot_out.reshape(block_count * block_rows, feature_count)
    copy_slot = jnp.zeros((copy_count,), jnp.int32).at[sort_order].set(destination).reshape(count_rows, TOPK)
    routed = jnp.zeros((count_rows, feature_count), jnp.float32)
    for choice_index in range(TOPK):
        picked = slot_out[copy_slot[:, choice_index]].astype(jnp.float32)
        routed = routed + gates[:, choice_index][:, None] * picked
    shared_out = gated_mlp(normed, shared_gate, shared_up, shared_down)
    mixed = (routed + shared_out).astype(jnp.bfloat16)
    load = counts.astype(jnp.float32) * (EXPERTS / (count_rows * TOPK))
    return (mixed, load)
```

```python
import functools

import jax
import jax.numpy as jnp
from jax import lax
from jax.experimental import pallas as pl
from jax.experimental.pallas import tpu as pltpu
from jax.sharding import PartitionSpec as P

F32 = jnp.float32
BF16 = jnp.bfloat16


def direct(
    n,
    eps,
    cap,
    tokens_hbm,
    routes,
    gates,
    gain,
    expert_gate,
    expert_up,
    expert_down,
    shared_gate,
    shared_up,
    shared_down,
    out,
    load,
    tokens,
    blocks,
    group_routes,
    every_routes,
    rows_in,
    hidden,
    results,
    returned,
    total,
    w_gate,
    w_up,
    w_down,
    s_gate,
    s_up,
    s_down,
    weight_sem,
    own_sem,
    route_send,
    route_recv,
    far_send,
    far_recv,
    token_send,
    token_recv,
    result_send,
    result_recv,
):
    me = lax.axis_index("tp")
    here = lax.axis_index("ep")
    rows, width = tokens.shape
    half = rows // 2
    chunk = rows // cap
    order = [lax.rem(me + i, n) for i in range(n)]

    barrier = pltpu.get_barrier_semaphore()
    planes = [lax.rem(here + i, eps) for i in range(1, eps)]
    for peer in order[1:]:
        pl.semaphore_signal(barrier, inc=1, device_id={"tp": peer})
    for plane in planes:
        pl.semaphore_signal(barrier, inc=1, device_id={"ep": plane})
    own_tokens = pltpu.make_async_copy(tokens_hbm, tokens, own_sem.at[1])
    own_tokens.start()

    weights = [
        pltpu.make_async_copy(src, dst, weight_sem.at[i])
        for i, (src, dst) in enumerate(
            [
                (expert_gate.at[0], w_gate),
                (expert_up.at[0], w_up),
                (expert_down.at[0], w_down),
                (shared_gate, s_gate),
                (shared_up, s_up),
                (shared_down, s_down),
            ]
        )
    ]
    for copy in weights:
        copy.start()
    own_routes = pltpu.make_async_copy(routes, group_routes.at[me], own_sem.at[0])
    own_routes.start()

    pl.semaphore_wait(barrier, n - 1 + eps - 1)

    pending = []
    for i, peer in enumerate(order[1:]):
        copy = pltpu.make_async_remote_copy(
            src_ref=routes,
            dst_ref=group_routes.at[me],
            send_sem=route_send.at[i],
            recv_sem=route_recv.at[me],
            device_id={"tp": peer},
        )
        copy.start()
        pending.append(copy)

    def part(ref, piece):
        return ref.at[pl.ds(piece * half, half)]

    def send(source, piece, slot, peer, number):
        copy = pltpu.make_async_remote_copy(
            src_ref=part(source, piece),
            dst_ref=part(blocks.at[slot], piece),
            send_sem=token_send.at[number],
            recv_sem=token_recv.at[slot, piece],
            device_id={"tp": peer},
        )
        copy.start()
        pending.append(copy)

    def landed(slot, piece):
        ref = part(blocks.at[slot], piece)
        pltpu.make_async_copy(ref, ref, token_recv.at[slot, piece]).wait()

    own_tokens.wait()
    for i, peer in enumerate(order[1:]):
        send(tokens, 0, me, peer, 2 * i)
        send(tokens, 1, me, peer, 2 * i + 1)

    earlier = (
        lax.broadcasted_iota(jnp.int32, (rows, rows), 0)
        < lax.broadcasted_iota(jnp.int32, (rows, rows), 1)
    ).astype(BF16)
    row_in_slot = lax.broadcasted_iota(jnp.int32, (cap, rows), 0)

    def normed_of(values):
        center = jnp.mean(values, axis=-1, keepdims=True)
        values = values - center
        spread = jnp.mean(jnp.square(values), axis=-1, keepdims=True)
        return (values * lax.rsqrt(spread + 1e-05) * gain[...]).astype(BF16)

    def gated(values, gate_ref, up_ref):
        gate_part = jnp.dot(values, gate_ref[...], preferred_element_type=F32)
        up_part = jnp.dot(values, up_ref[...], preferred_element_type=F32)
        return (gate_part * (1.0 / (1.0 + jnp.exp(-gate_part))) * up_part).astype(BF16)

    def gather(i, at):
        source = order[i]
        named = group_routes[source]
        member = (named[0:1] == me) | (named[1:2] == me)
        count = jnp.dot(
            jnp.broadcast_to(member.astype(F32), (8, rows)).astype(BF16),
            earlier,
            preferred_element_type=F32,
        )[0:1].astype(jnp.int32)
        slot = jnp.where(member, count, -1)
        pick = (row_in_slot == slot).astype(F32).astype(BF16)
        held = tokens[...] if i == 0 else blocks[source]
        taken = jnp.dot(pick, held, preferred_element_type=F32)
        rows_in[at * cap : (at + 1) * cap, :] = normed_of(taken)

    tile = 512

    def expert(members):
        count = len(members) * cap
        hidden[:count] = gated(rows_in[:count], w_gate, w_up)
        for at in range(0, width, tile):
            value = jnp.dot(
                hidden[:count], w_down[:, at : at + tile], preferred_element_type=F32
            ).astype(BF16)
            for g, i in enumerate(members):
                piece = value[g * cap : (g + 1) * cap]
                if i == 0:
                    returned[me, :, at : at + tile] = piece
                else:
                    results[i, :, at : at + tile] = piece
        for i in members:
            if i == 0:
                continue
            copy = pltpu.make_async_remote_copy(
                src_ref=results.at[i],
                dst_ref=returned.at[me],
                send_sem=result_send.at[i],
                recv_sem=result_recv.at[me],
                device_id={"tp": order[i]},
            )
            copy.start()
            pending.append(copy)

    own_routes.wait()
    for peer in order[1:]:
        ref = group_routes.at[peer]
        pltpu.make_async_copy(ref, ref, route_recv.at[peer]).wait()
    for i, plane in enumerate(planes):
        copy = pltpu.make_async_remote_copy(
            src_ref=group_routes,
            dst_ref=every_routes.at[here],
            send_sem=far_send.at[i],
            recv_sem=far_recv.at[here],
            device_id={"ep": plane},
        )
        copy.start()
        pending.append(copy)

    for copy in weights[:3]:
        copy.wait()
    for number in range(n // chunk):
        members = list(range(number * chunk, (number + 1) * chunk))
        for i in members:
            if i > 0:
                landed(order[i], 0)
                landed(order[i], 1)
            gather(i, i % chunk)
        expert(members)

    for copy in weights[3:]:
        copy.wait()
    rows_in[:rows] = normed_of(tokens[...].astype(F32))
    shared = gated(rows_in[:rows], s_gate, s_up)
    for at in range(0, width, tile):
        total[:, at : at + tile] = jnp.dot(
            shared, s_down[:, at : at + tile], preferred_element_type=F32
        )

    expert_ids = lax.broadcasted_iota(jnp.int32, (n, rows), 0)
    first, second = routes[0:1], routes[1:2]
    member = ((first == expert_ids) | (second == expert_ids)).astype(F32)
    ranks = jnp.dot(member.astype(BF16), earlier, preferred_element_type=F32)
    slots = [
        named * cap
        + jnp.sum(jnp.where(named == expert_ids, ranks, 0.0), axis=0, keepdims=True).astype(jnp.int32)
        for named in (first, second)
    ]

    def counted(ref_of, amount, start):
        def step(i, sums):
            named = ref_of(i)
            return (
                sums
                + (named[0:1] == expert_ids).astype(F32)
                + (named[1:2] == expert_ids).astype(F32)
            )

        return lax.fori_loop(0, amount, step, start)

    sums = counted(lambda i: group_routes[i], n, jnp.zeros((n, rows), F32))
    for plane in planes:
        ref = every_routes.at[plane]
        pltpu.make_async_copy(ref, ref, far_recv.at[plane]).wait()
        sums = counted(lambda i, plane=plane: every_routes[plane, i], n, sums)
    counts = lax.dot_general(
        jnp.ones((8, rows), F32),
        sums,
        (((1,), (1,)), ((), ())),
        precision=lax.Precision.HIGHEST,
        preferred_element_type=F32,
    )
    load[...] = counts[0:1, :] * (n / (rows * 2 * n * eps))

    columns = jnp.transpose(jnp.broadcast_to(gates[0:1], (8, rows))), jnp.transpose(
        jnp.broadcast_to(gates[1:2], (8, rows))
    )
    gate_of = [column[:, 0:1] for column in columns]
    parts = [list(range(at, at + chunk)) for at in range(0, n, chunk)]
    for members in parts:
        sources = [order[i] for i in members]
        picks = [
            jnp.transpose(
                jnp.concatenate(
                    [(row_in_slot + source * cap == slot).astype(F32) for source in sources], axis=0
                )
            ).astype(BF16)
            for slot in slots
        ]
        for i, source in zip(members, sources):
            if i > 0:
                ref = returned.at[source]
                pltpu.make_async_copy(ref, ref, result_recv.at[source]).wait()
        last = members is parts[-1]
        for at in range(0, width, tile):
            back = jnp.concatenate([returned[source, :, at : at + tile] for source in sources], axis=0)
            value = total[:, at : at + tile]
            for k in range(2):
                value = value + gate_of[k] * jnp.dot(picks[k], back, preferred_element_type=F32)
            if last:
                out[:, at : at + tile] = value.astype(BF16)
            else:
                total[:, at : at + tile] = value

    for copy in pending:
        copy.wait_send()


def square(
    eps,
    tokens_hbm,
    routes,
    gates,
    gain,
    expert_gate,
    expert_up,
    expert_down,
    shared_gate,
    shared_up,
    shared_down,
    out,
    load,
    blocks,
    group_routes,
    every_routes,
    near_gates,
    lanes,
    columns,
    normed,
    hidden,
    mine,
    lent,
    theirs,
    shared,
    merged,
    passed,
    back,
    base,
    w_gate,
    w_up,
    w_down,
    s_gate,
    s_up,
    s_down,
    weight_sem,
    own_sem,
    route_send,
    route_recv,
    far_send,
    far_recv,
    gate_recv,
    sent,
    token_recv,
    core_recv,
    result_recv,
    passed_recv,
    back_recv,
):
    n = 8
    me = lax.axis_index("tp")
    here = lax.axis_index("ep")
    rows, width = out.shape
    half, quarter = rows // 2, rows // 4
    piece = 16
    steps = half // piece
    core, xbit, ybit = me % 2, (me // 2) % 2, me // 4
    across = 1 - 2 * core
    sib = me + across
    nx = me + 2 * (1 - 2 * xbit)
    ny = me + 4 * (1 - 2 * ybit)
    nd = nx + 4 * (1 - 2 * ybit)
    others = [sib, nx, ny, nd, nx + across, ny + across, nd + across]

    barrier = pltpu.get_barrier_semaphore()
    planes = [lax.rem(here + i, eps) for i in range(1, eps)]
    for peer in others:
        pl.semaphore_signal(barrier, inc=1, device_id={"tp": peer})
    for plane in planes:
        pl.semaphore_signal(barrier, inc=1, device_id={"ep": plane})
    own_tokens = pltpu.make_async_copy(tokens_hbm, blocks.at[0], own_sem.at[1])
    own_tokens.start()
    weights = [
        pltpu.make_async_copy(src, dst, weight_sem.at[i])
        for i, (src, dst) in enumerate(
            [
                (expert_gate.at[0], w_gate),
                (expert_up.at[0], w_up),
                (expert_down.at[0], w_down),
                (shared_gate, s_gate),
                (shared_up, s_up),
                (shared_down, s_down),
            ]
        )
    ]
    for copy in weights:
        copy.start()
    own_routes = pltpu.make_async_copy(routes, group_routes.at[me], own_sem.at[0])
    own_routes.start()

    pl.semaphore_wait(barrier, n - 1 + eps - 1)

    pending = []

    def remote(source, target, send_sem, recv_sem, where):
        copy = pltpu.make_async_remote_copy(
            src_ref=source,
            dst_ref=target,
            send_sem=send_sem,
            recv_sem=recv_sem,
            device_id=where,
        )
        copy.start()
        pending.append(copy)

    numbers = iter(range(sent.shape[0]))

    def send(source, target, recv_sem, peer):
        remote(source, target, sent.at[next(numbers)], recv_sem, {"tp": peer})

    def arrived(ref, sem):
        pltpu.make_async_copy(ref, ref, sem).wait()

    def at_rows(ref, start, size):
        return ref.at[pl.ds(start, size)]

    def token_send(source, start, size, group, number, peer):
        send(
            at_rows(blocks.at[source], start, size),
            at_rows(blocks.at[group], start, size),
            token_recv.at[group, number],
            peer,
        )

    def lend(group, start, size, number):
        send(
            at_rows(blocks.at[group], start, size),
            at_rows(blocks.at[group + 4], start, size),
            core_recv.at[group, number],
            sib,
        )

    def landed(group, start, size, number):
        arrived(at_rows(blocks.at[group], start, size), token_recv.at[group, number])
        lend(group, start, size, number)

    def lent_in(group, start, size, number):
        arrived(at_rows(blocks.at[group + 4], start, size), core_recv.at[group, number])

    for i, peer in enumerate(others):
        remote(routes, group_routes.at[me], route_send.at[i], route_recv.at[me], {"tp": peer})
    for i, peer in enumerate([nx, ny, nd]):
        send(gates, near_gates.at[i], gate_recv.at[i], peer)
    own_tokens.wait()
    token_send(0, 0, half, 1, 0, nx)
    token_send(0, half, half, 1, 1, ny)
    token_send(0, half, quarter, 2, 2, nx)
    token_send(0, 0, quarter, 2, 0, ny)
    lend(0, 0, rows, 0)

    def norm(group):
        values = blocks[group].astype(F32)
        center = jnp.mean(values, axis=-1, keepdims=True)
        values = values - center
        spread = jnp.mean(jnp.square(values), axis=-1, keepdims=True)
        normed[...] = (values * lax.rsqrt(spread + 1e-05) * gain[...]).astype(BF16)

    def gated(values, gate_ref, up_ref):
        gate_part = jnp.dot(values, gate_ref[...], preferred_element_type=F32)
        up_part = jnp.dot(values, up_ref[...], preferred_element_type=F32)
        return (gate_part * (1.0 / (1.0 + jnp.exp(-gate_part))) * up_part).astype(BF16)

    tile = 512

    def expert(result):
        hidden[...] = gated(normed[...], w_gate, w_up)
        for at in range(0, width, tile):
            result[:, at : at + tile] = jnp.dot(
                hidden[...], w_down[:, at : at + tile], preferred_element_type=F32
            ).astype(BF16)

    def common(group):
        inner = gated(normed[...], s_gate, s_up)
        for at in range(0, width, tile):
            shared[group, :, at : at + tile] = jnp.dot(
                inner, s_down[:, at : at + tile], preferred_element_type=F32
            )

    def serve(group):
        norm(group + 4)
        expert(lent.at[group])
        send(lent.at[group], theirs.at[group], result_recv.at[group], sib)

    def named(ids):
        def test(route):
            hit = route == ids[0]
            for one in ids[1:]:
                hit = hit | (route == one)
            return hit

        return test

    def share(route, gate, test):
        first, second = test(route[0:1]), test(route[1:2])
        amount = first.astype(F32) + second.astype(F32)
        weight = jnp.where(first, gate[0:1], jnp.where(second, gate[1:2], 0.0))
        return amount, weight

    def store_columns(group, values):
        for i, value in enumerate(values):
            lanes[group, i : i + 1] = value
        columns[group] = jnp.transpose(lanes[group])

    lane = lax.broadcasted_iota(jnp.int32, (2, rows), 1)
    low = lane < half
    low_row = low[0:1]
    is_me, is_sib = named([me]), named([sib])
    on_x, on_y = named([nx, nx + across]), named([ny, ny + across])
    on_xd = named([nx, nx + across, nd, nd + across])
    on_yd = named([ny, ny + across, nd, nd + across])

    def coefficients(group, route, gate, relayed=False):
        mine_n, mine_g = share(route, gate, is_me)
        sib_n, sib_g = share(route, gate, is_sib)
        both = mine_n + sib_n
        if relayed:
            by_x, by_y = share(route, gate, on_x), share(route, gate, on_y)
            far_n, far_g = [jnp.where(low_row, a, b) for a, b in zip(by_x, by_y)]
            full = (both + far_n == 2.0) & (far_n < 2.0)
        else:
            full = both == 2.0
        values = [
            jnp.where(full, mine_g, mine_n),
            jnp.where(full, sib_g, sib_n),
            full.astype(F32),
        ]
        if relayed:
            values.append(jnp.where(full, far_g, 1.0))
        store_columns(group, values)

    def own_coefficients():
        route, gate = routes[...], gates[...]
        _, mine_g = share(route, gate, is_me)
        _, sib_g = share(route, gate, is_sib)
        x_low, x_high = share(route, gate, on_x), share(route, gate, on_xd)
        y_low, y_high = share(route, gate, on_yd), share(route, gate, on_y)
        x_n, x_g = [jnp.where(low_row, a, b) for a, b in zip(x_low, x_high)]
        y_n, y_g = [jnp.where(low_row, a, b) for a, b in zip(y_low, y_high)]
        done_x, done_y = x_n == 2.0, y_n == 2.0
        store_columns(
            0,
            [
                mine_g,
                sib_g,
                jnp.where(done_x | done_y, 0.0, 1.0),
                jnp.where(done_x, 1.0, x_g),
                jnp.where(done_y, 1.0, y_g),
            ],
        )

    def column(group, i, start, size):
        return columns[group, pl.ds(start, size), i : i + 1]

    def local_sum(group, start, size):
        where = pl.ds(start, size)
        return (
            column(group, 0, start, size) * mine[group, where].astype(F32)
            + column(group, 1, start, size) * theirs[group, where].astype(F32)
            + column(group, 2, start, size) * shared[group, where]
        )

    def into_sum(total, group):
        def step(i, carry):
            start = pl.multiple_of(i * piece, piece)
            total[pl.ds(start, piece)] = local_sum(group, start, piece)
            return carry

        lax.fori_loop(0, rows // piece, step, 0)

    def merge(group):
        def step(i, carry):
            start = pl.multiple_of(i * piece, piece)
            merged[group, pl.ds(start, piece)] = local_sum(group, start, piece).astype(BF16)
            return carry

        lax.fori_loop(0, rows // piece, step, 0)

    norm(0)
    for copy in weights[:3]:
        copy.wait()
    expert(mine.at[0])
    for copy in weights[3:]:
        copy.wait()
    common(0)
    lent_in(0, 0, rows, 0)
    serve(0)

    own_routes.wait()
    for peer in others:
        arrived(group_routes.at[peer], route_recv.at[peer])
    for i in range(3):
        arrived(near_gates.at[i], gate_recv.at[i])
    for i, plane in enumerate(planes):
        remote(group_routes, every_routes.at[here], far_send.at[i], far_recv.at[here], {"ep": plane})

    landed(1, 0, half, 0)
    token_send(1, 0, half, 3, 0, ny)
    landed(1, half, half, 1)
    token_send(1, half, half, 3, 1, nx)
    token_send(0, half + quarter, quarter, 2, 3, nx)
    token_send(0, quarter, quarter, 2, 1, ny)
    own_coefficients()
    x_route, y_route, d_route = group_routes[nx], group_routes[ny], group_routes[nd]
    x_gate, y_gate, d_gate = near_gates[0], near_gates[1], near_gates[2]
    coefficients(1, jnp.where(low, x_route, y_route), jnp.where(low, x_gate, y_gate))
    norm(1)
    expert(mine.at[1])
    common(1)
    lent_in(1, 0, half, 0)
    lent_in(1, half, half, 1)
    serve(1)
    landed(2, half, quarter, 2)
    landed(2, 0, quarter, 0)

    arrived(theirs.at[1], result_recv.at[1])
    merge(1)
    for first, peer in ((0, nx), (1, ny)):
        send(
            at_rows(merged.at[1], first * half, half),
            at_rows(back.at[first], first * half, half),
            back_recv.at[first, steps],
            peer,
        )
    coefficients(3, d_route, d_gate)
    coefficients(
        2,
        jnp.where(low, y_route, x_route),
        jnp.where(low, y_gate, x_gate),
        relayed=True,
    )
    arrived(theirs.at[0], result_recv.at[0])
    into_sum(base, 0)

    landed(3, 0, half, 0)
    landed(3, half, half, 1)
    norm(3)
    expert(mine.at[3])
    common(3)
    lent_in(3, 0, half, 0)
    lent_in(3, half, half, 1)
    serve(3)
    landed(2, half + quarter, quarter, 3)
    landed(2, quarter, quarter, 1)
    arrived(theirs.at[3], result_recv.at[3])
    merge(3)
    for step in range(steps):
        for first, peer in ((0, nx), (1, ny)):
            start = first * half + step * piece
            send(
                at_rows(merged.at[3], start, piece),
                at_rows(passed, start, piece),
                passed_recv.at[first, step],
                peer,
            )
    norm(2)
    expert(mine.at[2])
    common(2)
    for number in range(4):
        lent_in(2, number * quarter, quarter, number)
    serve(2)

    expert_ids = lax.broadcasted_iota(jnp.int32, (n, rows), 0)

    def counted(ref_of, amount, start):
        def step(i, sums):
            route = ref_of(i)
            return (
                sums
                + (route[0:1] == expert_ids).astype(F32)
                + (route[1:2] == expert_ids).astype(F32)
            )

        return lax.fori_loop(0, amount, step, start)

    sums = counted(lambda i: group_routes[i], n, jnp.zeros((n, rows), F32))
    for plane in planes:
        arrived(every_routes.at[plane], far_recv.at[plane])
        sums = counted(lambda i, plane=plane: every_routes[plane, i], n, sums)
    counts = lax.dot_general(
        jnp.ones((8, rows), F32),
        sums,
        (((1,), (1,)), ((), ())),
        precision=lax.Precision.HIGHEST,
        preferred_element_type=F32,
    )
    load[...] = counts[0:1, :] * (n / (rows * 2 * n * eps))

    arrived(theirs.at[2], result_recv.at[2])
    into_sum(shared.at[2], 2)

    for step in range(steps):
        for first, peer in ((1, nx), (0, ny)):
            start = first * half + step * piece
            where = pl.ds(start, piece)
            arrived(at_rows(passed, start, piece), passed_recv.at[first, step])
            merged[2, where] = (
                shared[2, where] + column(2, 3, start, piece) * passed[where].astype(F32)
            ).astype(BF16)
            send(
                at_rows(merged.at[2], start, piece),
                at_rows(back.at[1 - first], start, piece),
                back_recv.at[1 - first, step],
                peer,
            )

    for first in range(2):
        arrived(at_rows(back.at[first], first * half, half), back_recv.at[first, steps])

    def early(i, carry):
        for first in range(2):
            start = pl.multiple_of(first * half + i * piece, piece)
            where = pl.ds(start, piece)
            base[where] = base[where] + column(0, 3 + first, start, piece) * back[
                first, where
            ].astype(F32)
        return carry

    lax.fori_loop(0, steps, early, 0)

    for step in range(steps):
        for first in range(2):
            start = (1 - first) * half + step * piece
            where = pl.ds(start, piece)
            arrived(at_rows(back.at[first], start, piece), back_recv.at[first, step])
            out[where] = (
                base[where] + column(0, 3 + first, start, piece) * back[first, where].astype(F32)
            ).astype(BF16)

    for copy in pending:
        copy.wait_send()


def write_out(mixed, load, mixed_out, load_out, sem):
    copies = [
        pltpu.make_async_copy(mixed, mixed_out, sem.at[0]),
        pltpu.make_async_copy(load, load_out, sem.at[1]),
    ]
    for copy in copies:
        copy.start()
    for copy in copies:
        copy.wait()


def per_device(
    tokens,
    norm_gain,
    routes,
    gates,
    expert_gate,
    expert_up,
    expert_down,
    shared_gate,
    shared_up,
    shared_down,
):
    n, eps = lax.axis_size("tp"), lax.axis_size("ep")
    rows, width = tokens.shape
    top = routes.shape[1]
    cap = 2 * rows * top // n
    units = expert_gate.shape[2]
    vmem = pl.BlockSpec(memory_space=pltpu.VMEM)
    hbm = pl.BlockSpec(memory_space=pl.ANY)
    dma = pltpu.SemaphoreType.DMA
    weights = [
        pltpu.VMEM(expert_gate.shape[1:], BF16),
        pltpu.VMEM(expert_up.shape[1:], BF16),
        pltpu.VMEM(expert_down.shape[1:], BF16),
        pltpu.VMEM(shared_gate.shape, BF16),
        pltpu.VMEM(shared_up.shape, BF16),
        pltpu.VMEM(shared_down.shape, BF16),
        dma((6,)),
        dma((2,)),
        dma((n - 1,)),
        dma((n,)),
        dma((max(1, eps - 1),)),
        dma((eps,)),
    ]
    if n == 8:
        body = functools.partial(square, eps)
        scratch = [
            pltpu.VMEM((8, rows, width), BF16),
            pltpu.VMEM((n, top, rows), jnp.int32),
            pltpu.VMEM((eps, n, top, rows), jnp.int32),
            pltpu.VMEM((3, top, rows), F32),
            pltpu.VMEM((4, 8, rows), F32),
            pltpu.VMEM((4, rows, 8), F32),
            pltpu.VMEM((rows, width), BF16),
            pltpu.VMEM((rows, units), BF16),
            pltpu.VMEM((4, rows, width), BF16),
            pltpu.VMEM((4, rows, width), BF16),
            pltpu.VMEM((4, rows, width), BF16),
            pltpu.VMEM((4, rows, width), F32),
            pltpu.VMEM((4, rows, width), BF16),
            pltpu.VMEM((rows, width), BF16),
            pltpu.VMEM((2, rows, width), BF16),
            pltpu.VMEM((rows, width), F32),
            *weights,
            dma((3,)),
            dma((26 + rows // 8,)),
            dma((4, 4)),
            dma((4, 4)),
            dma((4,)),
            dma((2, rows // 32)),
            dma((2, rows // 32 + 1)),
        ]
    else:
        body = functools.partial(direct, n, eps, cap)
        scratch = [
            pltpu.VMEM((rows, width), BF16),
            pltpu.VMEM((n, rows, width), BF16),
            pltpu.VMEM((n, top, rows), jnp.int32),
            pltpu.VMEM((eps, n, top, rows), jnp.int32),
            pltpu.VMEM((rows, width), BF16),
            pltpu.VMEM((rows, units), BF16),
            pltpu.VMEM((n, cap, width), BF16),
            pltpu.VMEM((n, cap, width), BF16),
            pltpu.VMEM((rows, width), F32),
            *weights,
            dma((2 * (n - 1),)),
            dma((n, 2)),
            dma((n,)),
            dma((n,)),
        ]
    mixed, load = pl.pallas_call(
        body,
        out_shape=(
            pltpu.VMEM((rows, width), BF16),
            pltpu.VMEM((1, n), F32),
        ),
        in_specs=[hbm] + [vmem] * 3 + [hbm] * 6,
        out_specs=(vmem, vmem),
        scratch_shapes=scratch,
        compiler_params=pltpu.CompilerParams(
            collective_id=0, has_side_effects=True
        ),
    )(
        tokens,
        routes.T,
        gates.T,
        norm_gain.reshape(1, width),
        expert_gate,
        expert_up,
        expert_down,
        shared_gate,
        shared_up,
        shared_down,
    )
    mixed, load = pl.pallas_call(
        write_out,
        out_shape=(
            jax.ShapeDtypeStruct((rows, width), BF16),
            jax.ShapeDtypeStruct((1, n), F32),
        ),
        in_specs=[vmem] * 2,
        out_specs=(hbm, hbm),
        scratch_shapes=[dma((2,))],
        compiler_params=pltpu.CompilerParams(vmem_limit_bytes=1 << 20),
    )(mixed, load)
    return mixed, load.reshape(n)


def solution(mesh):
    placed = (
        P(("ep", "tp"), None),
        P(),
        P(("ep", "tp"), None),
        P(("ep", "tp"), None),
        P("tp", None, None),
        P("tp", None, None),
        P("tp", None, None),
        P(),
        P(),
        P(),
    )
    return jax.shard_map(
        per_device,
        mesh=mesh,
        in_specs=placed,
        out_specs=(P(("ep", "tp"), None), P()),
        check_vma=False,
    )
```

```python
import functools

import jax
import jax.numpy as jnp
from jax import lax
from jax.experimental import pallas as pl
from jax.experimental.pallas import tpu as pltpu
from jax.sharding import PartitionSpec as P

F32 = jnp.float32
BF16 = jnp.bfloat16


def direct(
    n,
    eps,
    cap,
    tokens_hbm,
    routes,
    gates,
    gain,
    expert_gate,
    expert_up,
    expert_down,
    shared_gate,
    shared_up,
    shared_down,
    out,
    load,
    tokens,
    blocks,
    group_routes,
    every_routes,
    rows_in,
    hidden,
    results,
    returned,
    total,
    w_gate,
    w_up,
    w_down,
    s_gate,
    s_up,
    s_down,
    weight_sem,
    own_sem,
    route_send,
    route_recv,
    far_send,
    far_recv,
    token_send,
    token_recv,
    result_send,
    result_recv,
):
    me = lax.axis_index("tp")
    here = lax.axis_index("ep")
    rows, width = tokens.shape
    half = rows // 2
    chunk = rows // cap
    order = [lax.rem(me + i, n) for i in range(n)]

    barrier = pltpu.get_barrier_semaphore()
    planes = [lax.rem(here + i, eps) for i in range(1, eps)]
    for peer in order[1:]:
        pl.semaphore_signal(barrier, inc=1, device_id={"tp": peer})
    for plane in planes:
        pl.semaphore_signal(barrier, inc=1, device_id={"ep": plane})
    own_tokens = pltpu.make_async_copy(tokens_hbm, tokens, own_sem.at[1])
    own_tokens.start()

    weights = [
        pltpu.make_async_copy(src, dst, weight_sem.at[i])
        for i, (src, dst) in enumerate(
            [
                (expert_gate.at[0], w_gate),
                (expert_up.at[0], w_up),
                (expert_down.at[0], w_down),
                (shared_gate, s_gate),
                (shared_up, s_up),
                (shared_down, s_down),
            ]
        )
    ]
    for copy in weights:
        copy.start()
    own_routes = pltpu.make_async_copy(routes, group_routes.at[me], own_sem.at[0])
    own_routes.start()

    pl.semaphore_wait(barrier, n - 1 + eps - 1)

    pending = []
    for i, peer in enumerate(order[1:]):
        copy = pltpu.make_async_remote_copy(
            src_ref=routes,
            dst_ref=group_routes.at[me],
            send_sem=route_send.at[i],
            recv_sem=route_recv.at[me],
            device_id={"tp": peer},
        )
        copy.start()
        pending.append(copy)

    def part(ref, piece):
        return ref.at[pl.ds(piece * half, half)]

    def send(source, piece, slot, peer, number):
        copy = pltpu.make_async_remote_copy(
            src_ref=part(source, piece),
            dst_ref=part(blocks.at[slot], piece),
            send_sem=token_send.at[number],
            recv_sem=token_recv.at[slot, piece],
            device_id={"tp": peer},
        )
        copy.start()
        pending.append(copy)

    def landed(slot, piece):
        ref = part(blocks.at[slot], piece)
        pltpu.make_async_copy(ref, ref, token_recv.at[slot, piece]).wait()

    own_tokens.wait()
    for i, peer in enumerate(order[1:]):
        send(tokens, 0, me, peer, 2 * i)
        send(tokens, 1, me, peer, 2 * i + 1)

    earlier = (
        lax.broadcasted_iota(jnp.int32, (rows, rows), 0)
        < lax.broadcasted_iota(jnp.int32, (rows, rows), 1)
    ).astype(BF16)
    row_in_slot = lax.broadcasted_iota(jnp.int32, (cap, rows), 0)

    def normed_of(values):
        center = jnp.mean(values, axis=-1, keepdims=True)
        values = values - center
        spread = jnp.mean(jnp.square(values), axis=-1, keepdims=True)
        return (values * lax.rsqrt(spread + 1e-05) * gain[...]).astype(BF16)

    def gated(values, gate_ref, up_ref):
        gate_part = jnp.dot(values, gate_ref[...], preferred_element_type=F32)
        up_part = jnp.dot(values, up_ref[...], preferred_element_type=F32)
        return (gate_part * (1.0 / (1.0 + jnp.exp(-gate_part))) * up_part).astype(BF16)

    def gather(i, at):
        source = order[i]
        named = group_routes[source]
        member = (named[0:1] == me) | (named[1:2] == me)
        count = jnp.dot(
            jnp.broadcast_to(member.astype(F32), (8, rows)).astype(BF16),
            earlier,
            preferred_element_type=F32,
        )[0:1].astype(jnp.int32)
        slot = jnp.where(member, count, -1)
        pick = (row_in_slot == slot).astype(F32).astype(BF16)
        held = tokens[...] if i == 0 else blocks[source]
        taken = jnp.dot(pick, held, preferred_element_type=F32)
        rows_in[at * cap : (at + 1) * cap, :] = normed_of(taken)

    tile = 512

    def expert(members):
        count = len(members) * cap
        hidden[:count] = gated(rows_in[:count], w_gate, w_up)
        for at in range(0, width, tile):
            value = jnp.dot(
                hidden[:count], w_down[:, at : at + tile], preferred_element_type=F32
            ).astype(BF16)
            for g, i in enumerate(members):
                piece = value[g * cap : (g + 1) * cap]
                if i == 0:
                    returned[me, :, at : at + tile] = piece
                else:
                    results[i, :, at : at + tile] = piece
        for i in members:
            if i == 0:
                continue
            copy = pltpu.make_async_remote_copy(
                src_ref=results.at[i],
                dst_ref=returned.at[me],
                send_sem=result_send.at[i],
                recv_sem=result_recv.at[me],
                device_id={"tp": order[i]},
            )
            copy.start()
            pending.append(copy)

    own_routes.wait()
    for peer in order[1:]:
        ref = group_routes.at[peer]
        pltpu.make_async_copy(ref, ref, route_recv.at[peer]).wait()
    for i, plane in enumerate(planes):
        copy = pltpu.make_async_remote_copy(
            src_ref=group_routes,
            dst_ref=every_routes.at[here],
            send_sem=far_send.at[i],
            recv_sem=far_recv.at[here],
            device_id={"ep": plane},
        )
        copy.start()
        pending.append(copy)

    for copy in weights[:3]:
        copy.wait()
    for number in range(n // chunk):
        members = list(range(number * chunk, (number + 1) * chunk))
        for i in members:
            if i > 0:
                landed(order[i], 0)
                landed(order[i], 1)
            gather(i, i % chunk)
        expert(members)

    for copy in weights[3:]:
        copy.wait()
    rows_in[:rows] = normed_of(tokens[...].astype(F32))
    shared = gated(rows_in[:rows], s_gate, s_up)
    for at in range(0, width, tile):
        total[:, at : at + tile] = jnp.dot(
            shared, s_down[:, at : at + tile], preferred_element_type=F32
        )

    expert_ids = lax.broadcasted_iota(jnp.int32, (n, rows), 0)
    first, second = routes[0:1], routes[1:2]
    member = ((first == expert_ids) | (second == expert_ids)).astype(F32)
    ranks = jnp.dot(member.astype(BF16), earlier, preferred_element_type=F32)
    slots = [
        named * cap
        + jnp.sum(jnp.where(named == expert_ids, ranks, 0.0), axis=0, keepdims=True).astype(jnp.int32)
        for named in (first, second)
    ]

    def counted(ref_of, amount, start):
        def step(i, sums):
            named = ref_of(i)
            return (
                sums
                + (named[0:1] == expert_ids).astype(F32)
                + (named[1:2] == expert_ids).astype(F32)
            )

        return lax.fori_loop(0, amount, step, start)

    sums = counted(lambda i: group_routes[i], n, jnp.zeros((n, rows), F32))
    for plane in planes:
        ref = every_routes.at[plane]
        pltpu.make_async_copy(ref, ref, far_recv.at[plane]).wait()
        sums = counted(lambda i, plane=plane: every_routes[plane, i], n, sums)
    counts = lax.dot_general(
        jnp.ones((8, rows), F32),
        sums,
        (((1,), (1,)), ((), ())),
        precision=lax.Precision.HIGHEST,
        preferred_element_type=F32,
    )
    load[...] = counts[0:1, :] * (n / (rows * 2 * n * eps))

    columns = jnp.transpose(jnp.broadcast_to(gates[0:1], (8, rows))), jnp.transpose(
        jnp.broadcast_to(gates[1:2], (8, rows))
    )
    gate_of = [column[:, 0:1] for column in columns]
    parts = [list(range(at, at + chunk)) for at in range(0, n, chunk)]
    for members in parts:
        sources = [order[i] for i in members]
        picks = [
            jnp.transpose(
                jnp.concatenate(
                    [(row_in_slot + source * cap == slot).astype(F32) for source in sources], axis=0
                )
            ).astype(BF16)
            for slot in slots
        ]
        for i, source in zip(members, sources):
            if i > 0:
                ref = returned.at[source]
                pltpu.make_async_copy(ref, ref, result_recv.at[source]).wait()
        last = members is parts[-1]
        for at in range(0, width, tile):
            back = jnp.concatenate([returned[source, :, at : at + tile] for source in sources], axis=0)
            value = total[:, at : at + tile]
            for k in range(2):
                value = value + gate_of[k] * jnp.dot(picks[k], back, preferred_element_type=F32)
            if last:
                out[:, at : at + tile] = value.astype(BF16)
            else:
                total[:, at : at + tile] = value

    for copy in pending:
        copy.wait_send()


def square(
    eps,
    tokens_hbm,
    routes_hbm,
    gates_hbm,
    gain_hbm,
    expert_gate,
    expert_up,
    expert_down,
    shared_gate,
    shared_up,
    shared_down,
    out,
    load,
    blocks,
    routes,
    gates,
    gain,
    near_routes,
    near_gates,
    tally,
    lanes,
    columns,
    normed,
    hidden,
    mine,
    lent,
    theirs,
    shared,
    merged,
    passed,
    back,
    base,
    w_in,
    w_down,
    s_in,
    s_down,
    own_sem,
    sent,
    meta_recv,
    tally_recv,
    token_recv,
    core_recv,
    result_recv,
    passed_recv,
    back_recv,
):
    n = 8
    me = lax.axis_index("tp")
    here = lax.axis_index("ep")
    rows, width = out.shape
    half, quarter = rows // 2, rows // 4
    piece = 16
    steps = half // piece
    core, xbit, ybit = me % 2, (me // 2) % 2, me // 4
    across = 1 - 2 * core
    sib = me + across
    nx = me + 2 * (1 - 2 * xbit)
    ny = me + 4 * (1 - 2 * ybit)
    nd = nx + 4 * (1 - 2 * ybit)
    column_head = me == 0
    below, above = column_head & (here > 0), column_head & (here < eps - 1)

    barrier = pltpu.get_barrier_semaphore()
    for peer in (sib, nx, ny):
        pl.semaphore_signal(barrier, inc=1, device_id={"tp": peer})

    @pl.when(below)
    def _():
        pl.semaphore_signal(barrier, inc=1, device_id={"ep": here - 1})

    @pl.when(above)
    def _():
        pl.semaphore_signal(barrier, inc=1, device_id={"ep": here + 1})

    copies = [
        (0, tokens_hbm, blocks.at[0]),
        (1, routes_hbm, routes),
        (2, gates_hbm, gates),
        (3, gain_hbm, gain),
        (4, expert_gate.at[0], w_in.at[0]),
        (4, expert_up.at[0], w_in.at[1]),
        (5, expert_down.at[0], w_down),
        (6, shared_gate, s_in.at[0]),
        (6, shared_up, s_in.at[1]),
        (7, shared_down, s_down),
    ]
    for number, source, target in copies:
        pltpu.make_async_copy(source, target, own_sem.at[number]).start()

    def arrived(ref, sem):
        pltpu.make_async_copy(ref, ref, sem).wait()

    pl.semaphore_wait(barrier, 3 + jnp.where(below, 1, 0) + jnp.where(above, 1, 0))

    def send(source, target, send_sem, recv_sem, where):
        pltpu.make_async_remote_copy(
            src_ref=source,
            dst_ref=target,
            send_sem=send_sem,
            recv_sem=recv_sem,
            device_id=where,
        ).start()

    def at_rows(ref, start, size):
        return ref.at[pl.ds(start, size)]

    def link(source, target, start, size, recv_sem, peer):
        send(
            at_rows(source, start, size),
            at_rows(target, start, size),
            sent.at[0],
            recv_sem,
            {"tp": peer},
        )

    def token_send(source, start, size, group, number, peer):
        link(blocks.at[source], blocks.at[group], start, size, token_recv.at[number], peer)

    def lend(group, start, size):
        send(
            at_rows(blocks.at[group], start, size),
            at_rows(blocks.at[group + 4], start, size),
            sent.at[1],
            core_recv.at[group],
            {"tp": sib},
        )

    def landed(group, start, size, number):
        arrived(at_rows(blocks.at[group], start, size), token_recv.at[number])

    arrived(routes, own_sem.at[1])
    arrived(gates, own_sem.at[2])
    for i, peer in enumerate((nx, ny)):
        send(routes, near_routes.at[i], sent.at[2], meta_recv.at[0], {"tp": peer})
        send(gates, near_gates.at[i], sent.at[2], meta_recv.at[0], {"tp": peer})
    arrived(blocks.at[0], own_sem.at[0])
    token_send(0, 0, half, 1, 0, nx)
    token_send(0, half, half, 1, 1, ny)
    lend(0, 0, rows)

    expert_ids = lax.broadcasted_iota(jnp.int32, (n, rows), 0)

    def tallied(route):
        return (route[0:1] == expert_ids).astype(F32) + (route[1:2] == expert_ids).astype(F32)

    def tally_send(source, target, number, recv, where):
        send(tally.at[source], tally.at[target], sent.at[number], tally_recv.at[recv], where)

    def along_column(rounds):
        for r in rounds:

            @pl.when(column_head & (here == r))
            def _():
                value = tally[2]
                if r > 0:
                    arrived(tally.at[3], tally_recv.at[1])
                    value = value + tally[3]
                tally[5] = value
                if r < eps - 1:
                    tally_send(5, 3, 5, 1, {"ep": here + 1})

            @pl.when(column_head & (here == eps - 1 - r))
            def _():
                value = tally[2]
                if r > 0:
                    arrived(tally.at[4], tally_recv.at[2])
                    value = value + tally[4]
                tally[6] = value
                if r < eps - 1:
                    tally_send(6, 4, 6, 2, {"ep": here - 1})

    hand = {
        7: (core == 0, sib),
        8: (column_head, nx),
        9: ((core == 0) & (ybit == 0), ny),
    }
    handers = [
        (column_head, (7, 8, 9)),
        ((core == 0) & (xbit == 1) & (ybit == 0), (7, 9)),
        ((core == 0) & (xbit == 0) & (ybit == 1), (7,)),
        ((core == 0) & (xbit == 1) & (ybit == 1), (7,)),
        (core == 1, ()),
    ]

    def hand_on(number):
        test, numbers = handers[number]

        @pl.when(test)
        def _():
            if number > 0:
                arrived(tally.at[7], tally_recv.at[3])
            for i in numbers:
                tally_send(7, 7, i, 3, {"tp": hand[i][1]})

    def norm(group, slot=0):
        values = blocks[group].astype(F32)
        center = jnp.mean(values, axis=-1, keepdims=True)
        values = values - center
        spread = jnp.mean(jnp.square(values), axis=-1, keepdims=True)
        normed[slot] = (values * lax.rsqrt(spread + 1e-05) * gain[...]).astype(BF16)

    def gated(values, gate_ref, up_ref):
        gate_part = jnp.dot(values, gate_ref[...], preferred_element_type=F32)
        up_part = jnp.dot(values, up_ref[...], preferred_element_type=F32)
        return (gate_part * (1.0 / (1.0 + jnp.exp(-gate_part))) * up_part).astype(BF16)

    tile = 512

    def expert(result, slot=0):
        hidden[...] = gated(normed[slot], w_in.at[0], w_in.at[1])
        for at in range(0, width, tile):
            result[:, at : at + tile] = jnp.dot(
                hidden[...], w_down[:, at : at + tile], preferred_element_type=F32
            ).astype(BF16)

    def common(group):
        inner = gated(normed[0], s_in.at[0], s_in.at[1])
        for at in range(0, width, tile):
            shared[group, :, at : at + tile] = jnp.dot(
                inner, s_down[:, at : at + tile], preferred_element_type=F32
            )

    def serve(group):
        arrived(blocks.at[group + 4], core_recv.at[group])
        norm(group + 4, 1)
        expert(lent.at[group], 1)
        send(lent.at[group], theirs.at[group], sent.at[1], result_recv.at[group], {"tp": sib})

    def named(ids):
        def test(route):
            hit = route == ids[0]
            for one in ids[1:]:
                hit = hit | (route == one)
            return hit

        return test

    def share(route, gate, test):
        first, second = test(route[0:1]), test(route[1:2])
        amount = first.astype(F32) + second.astype(F32)
        weight = jnp.where(first, gate[0:1], jnp.where(second, gate[1:2], 0.0))
        return amount, weight

    def store_columns(group, values):
        for i, value in enumerate(values):
            lanes[group, i : i + 1] = value
        columns[group] = jnp.transpose(lanes[group])

    lane = lax.broadcasted_iota(jnp.int32, (2, rows), 1)
    low = lane < half
    low_row = low[0:1]
    is_me, is_sib = named([me]), named([sib])
    on_x, on_y = named([nx, nx + across]), named([ny, ny + across])
    on_xd = named([nx, nx + across, nd, nd + across])
    on_yd = named([ny, ny + across, nd, nd + across])

    def coefficients(group, route, gate, relayed=False):
        mine_n, mine_g = share(route, gate, is_me)
        sib_n, sib_g = share(route, gate, is_sib)
        both = mine_n + sib_n
        if relayed:
            by_x, by_y = share(route, gate, on_x), share(route, gate, on_y)
            far_n, far_g = [jnp.where(low_row, a, b) for a, b in zip(by_x, by_y)]
            full = (both + far_n == 2.0) & (far_n < 2.0)
        else:
            full = both == 2.0
        values = [
            jnp.where(full, mine_g, mine_n),
            jnp.where(full, sib_g, sib_n),
            full.astype(F32),
        ]
        if relayed:
            values.append(jnp.where(full, far_g, 1.0))
        store_columns(group, values)

    def own_coefficients():
        route, gate = routes[...], gates[...]
        _, mine_g = share(route, gate, is_me)
        _, sib_g = share(route, gate, is_sib)
        x_low, x_high = share(route, gate, on_x), share(route, gate, on_xd)
        y_low, y_high = share(route, gate, on_yd), share(route, gate, on_y)
        x_n, x_g = [jnp.where(low_row, a, b) for a, b in zip(x_low, x_high)]
        y_n, y_g = [jnp.where(low_row, a, b) for a, b in zip(y_low, y_high)]
        done_x, done_y = x_n == 2.0, y_n == 2.0
        store_columns(
            0,
            [
                mine_g,
                sib_g,
                jnp.where(done_x | done_y, 0.0, 1.0),
                jnp.where(done_x, 1.0, x_g),
                jnp.where(done_y, 1.0, y_g),
            ],
        )

    def column(group, i, start, size):
        return columns[group, pl.ds(start, size), i : i + 1]

    def local_sum(group, start, size):
        where = pl.ds(start, size)
        return (
            column(group, 0, start, size) * mine[group, where].astype(F32)
            + column(group, 1, start, size) * theirs[group, where].astype(F32)
            + column(group, 2, start, size) * shared[group, where]
        )

    def into_sum(total, group):
        def step(i, carry):
            start = pl.multiple_of(i * piece, piece)
            total[pl.ds(start, piece)] = local_sum(group, start, piece)
            return carry

        lax.fori_loop(0, rows // piece, step, 0)

    def merge(group, target_of, recv_of):
        for step in range(steps):
            for first, peer in ((0, nx), (1, ny)):
                start = first * half + step * piece
                merged[group, pl.ds(start, piece)] = local_sum(group, start, piece).astype(BF16)
                link(merged.at[group], target_of(first), start, piece, recv_of(step), peer)

    arrived(gain, own_sem.at[3])
    norm(0)
    arrived(w_in, own_sem.at[4])
    arrived(w_down, own_sem.at[5])
    expert(mine.at[0])
    arrived(s_in, own_sem.at[6])
    arrived(s_down, own_sem.at[7])
    common(0)
    serve(0)

    arrived(tally.at[0], meta_recv.at[0])
    arrived(tally.at[0], sent.at[2])
    send(near_routes.at[0], near_routes.at[2], sent.at[3], meta_recv.at[1], {"tp": ny})
    send(near_gates.at[0], near_gates.at[2], sent.at[3], meta_recv.at[1], {"tp": ny})
    token_send(0, half, quarter, 2, 2, nx)
    token_send(0, 0, quarter, 2, 2, ny)
    own_coefficients()
    x_route, y_route = near_routes[0], near_routes[1]
    x_gate, y_gate = near_gates[0], near_gates[1]
    coefficients(1, jnp.where(low, x_route, y_route), jnp.where(low, x_gate, y_gate))
    coefficients(
        2,
        jnp.where(low, y_route, x_route),
        jnp.where(low, y_gate, x_gate),
        relayed=True,
    )

    landed(1, 0, half, 0)
    token_send(1, 0, quarter, 3, 4, ny)
    token_send(1, quarter, quarter, 3, 5, ny)
    lend(1, 0, half)
    landed(1, half, half, 1)
    token_send(1, half, quarter, 3, 4, nx)
    token_send(1, half + quarter, quarter, 3, 5, nx)
    lend(1, half, half)
    token_send(0, half + quarter, quarter, 2, 3, nx)
    token_send(0, quarter, quarter, 2, 3, ny)
    arrived(at_rows(near_routes, 0, 2), meta_recv.at[1])
    d_route = near_routes[2]
    tally[0] = tallied(routes[...]) + tallied(x_route) + tallied(y_route) + tallied(d_route)
    tally_send(0, 1, 4, 0, {"tp": sib})
    norm(1)
    expert(mine.at[1])
    arrived(tally.at[1], tally_recv.at[0])
    tally[2] = tally[0] + tally[1]
    rounds = list(range(eps))
    along_column(rounds[:1])
    serve(1)
    common(1)
    coefficients(3, d_route, near_gates[2])
    arrived(theirs.at[0], result_recv.at[0])
    into_sum(base, 0)
    landed(2, 0, half, 2)
    lend(2, half, quarter)
    lend(2, 0, quarter)
    along_column(rounds[1:2])
    arrived(theirs.at[1], result_recv.at[1])
    merge(1, lambda first: back.at[first], lambda step: back_recv.at[steps])

    landed(3, 0, half, 4)
    lend(3, 0, quarter)
    lend(3, half, quarter)
    landed(3, 0, half, 5)
    lend(3, quarter, quarter)
    lend(3, half + quarter, quarter)
    along_column(rounds[2:3])
    norm(3)
    expert(mine.at[3])
    serve(3)
    common(3)
    landed(2, 0, half, 3)
    lend(2, half + quarter, quarter)
    lend(2, quarter, quarter)
    along_column(rounds[3:])

    @pl.when(column_head)
    def _():
        tally[7] = tally[5] + tally[6] - tally[2]

    hand_on(0)
    arrived(theirs.at[3], result_recv.at[3])
    merge(3, lambda first: passed, lambda step: passed_recv.at[step])
    serve(2)
    norm(2)
    expert(mine.at[2])
    common(2)
    arrived(theirs.at[2], result_recv.at[2])
    into_sum(shared.at[2], 2)
    hand_on(1)
    hand_on(2)

    for step in range(steps):
        arrived(at_rows(passed, 0, 2 * piece), passed_recv.at[step])
        for first, peer in ((1, nx), (0, ny)):
            start = first * half + step * piece
            where = pl.ds(start, piece)
            merged[2, where] = (
                shared[2, where] + column(2, 3, start, piece) * passed[where].astype(F32)
            ).astype(BF16)
            link(merged.at[2], back.at[1 - first], start, piece, back_recv.at[step], peer)

    arrived(at_rows(back.at[0], 0, rows), back_recv.at[steps])

    def early(i, carry):
        for first in range(2):
            start = pl.multiple_of(first * half + i * piece, piece)
            where = pl.ds(start, piece)
            base[where] = base[where] + column(0, 3 + first, start, piece) * back[
                first, where
            ].astype(F32)
        return carry

    lax.fori_loop(0, steps, early, 0)

    hand_on(3)
    hand_on(4)
    counts = lax.dot_general(
        jnp.ones((8, rows), F32),
        tally[7],
        (((1,), (1,)), ((), ())),
        precision=lax.Precision.HIGHEST,
        preferred_element_type=F32,
    )
    load[...] = counts[0:1, :] * (n / (rows * 2 * n * eps))

    for step in range(steps):
        arrived(at_rows(back.at[0], 0, 2 * piece), back_recv.at[step])
        for first in range(2):
            start = (1 - first) * half + step * piece
            where = pl.ds(start, piece)
            out[where] = (
                base[where] + column(0, 3 + first, start, piece) * back[first, where].astype(F32)
            ).astype(BF16)

    arrived(at_rows(blocks, 0, 6), sent.at[0])
    arrived(blocks, sent.at[1])
    arrived(at_rows(near_routes, 0, 2), sent.at[3])
    arrived(tally.at[0], sent.at[4])
    for number, test in ((5, above), (6, below), *((i, hand[i][0]) for i in hand)):

        @pl.when(test)
        def _():
            arrived(tally.at[0], sent.at[number])


def write_out(mixed, load, mixed_out, load_out, sem):
    copies = [
        pltpu.make_async_copy(mixed, mixed_out, sem.at[0]),
        pltpu.make_async_copy(load, load_out, sem.at[1]),
    ]
    for copy in copies:
        copy.start()
    for copy in copies:
        copy.wait()


def per_device(
    tokens,
    norm_gain,
    routes,
    gates,
    expert_gate,
    expert_up,
    expert_down,
    shared_gate,
    shared_up,
    shared_down,
):
    n, eps = lax.axis_size("tp"), lax.axis_size("ep")
    rows, width = tokens.shape
    top = routes.shape[1]
    cap = 2 * rows * top // n
    units = expert_gate.shape[2]
    vmem = pl.BlockSpec(memory_space=pltpu.VMEM)
    hbm = pl.BlockSpec(memory_space=pl.ANY)
    dma = pltpu.SemaphoreType.DMA
    if n == 8:
        body = functools.partial(square, eps)
        small = hbm
        scratch = [
            pltpu.VMEM((8, rows, width), BF16),
            pltpu.VMEM((top, rows), jnp.int32),
            pltpu.VMEM((top, rows), F32),
            pltpu.VMEM((1, width), F32),
            pltpu.VMEM((3, top, rows), jnp.int32),
            pltpu.VMEM((3, top, rows), F32),
            pltpu.VMEM((8, n, rows), F32),
            pltpu.VMEM((4, 8, rows), F32),
            pltpu.VMEM((4, rows, 8), F32),
            pltpu.VMEM((2, rows, width), BF16),
            pltpu.VMEM((rows, units), BF16),
            pltpu.VMEM((4, rows, width), BF16),
            pltpu.VMEM((4, rows, width), BF16),
            pltpu.VMEM((4, rows, width), BF16),
            pltpu.VMEM((4, rows, width), F32),
            pltpu.VMEM((4, rows, width), BF16),
            pltpu.VMEM((rows, width), BF16),
            pltpu.VMEM((2, rows, width), BF16),
            pltpu.VMEM((rows, width), F32),
            pltpu.VMEM((2, *expert_gate.shape[1:]), BF16),
            pltpu.VMEM(expert_down.shape[1:], BF16),
            pltpu.VMEM((2, *shared_gate.shape), BF16),
            pltpu.VMEM(shared_down.shape, BF16),
            dma((8,)),
            dma((10,)),
            dma((2,)),
            dma((4,)),
            dma((6,)),
            dma((4,)),
            dma((4,)),
            dma((rows // 32,)),
            dma((rows // 32 + 1,)),
        ]
    else:
        body = functools.partial(direct, n, eps, cap)
        small = vmem
        scratch = [
            pltpu.VMEM((rows, width), BF16),
            pltpu.VMEM((n, rows, width), BF16),
            pltpu.VMEM((n, top, rows), jnp.int32),
            pltpu.VMEM((eps, n, top, rows), jnp.int32),
            pltpu.VMEM((rows, width), BF16),
            pltpu.VMEM((rows, units), BF16),
            pltpu.VMEM((n, cap, width), BF16),
            pltpu.VMEM((n, cap, width), BF16),
            pltpu.VMEM((rows, width), F32),
            pltpu.VMEM(expert_gate.shape[1:], BF16),
            pltpu.VMEM(expert_up.shape[1:], BF16),
            pltpu.VMEM(expert_down.shape[1:], BF16),
            pltpu.VMEM(shared_gate.shape, BF16),
            pltpu.VMEM(shared_up.shape, BF16),
            pltpu.VMEM(shared_down.shape, BF16),
            dma((6,)),
            dma((2,)),
            dma((n - 1,)),
            dma((n,)),
            dma((max(1, eps - 1),)),
            dma((eps,)),
            dma((2 * (n - 1),)),
            dma((n, 2)),
            dma((n,)),
            dma((n,)),
        ]
    mixed, load = pl.pallas_call(
        body,
        out_shape=(
            pltpu.VMEM((rows, width), BF16),
            pltpu.VMEM((1, n), F32),
        ),
        in_specs=[hbm] + [small] * 3 + [hbm] * 6,
        out_specs=(vmem, vmem),
        scratch_shapes=scratch,
        compiler_params=pltpu.CompilerParams(
            collective_id=0, has_side_effects=True
        ),
    )(
        tokens,
        routes.T,
        gates.T,
        norm_gain.reshape(1, width),
        expert_gate,
        expert_up,
        expert_down,
        shared_gate,
        shared_up,
        shared_down,
    )
    mixed, load = pl.pallas_call(
        write_out,
        out_shape=(
            jax.ShapeDtypeStruct((rows, width), BF16),
            jax.ShapeDtypeStruct((1, n), F32),
        ),
        in_specs=[vmem] * 2,
        out_specs=(hbm, hbm),
        scratch_shapes=[dma((2,))],
        compiler_params=pltpu.CompilerParams(vmem_limit_bytes=1 << 20),
    )(mixed, load)
    return mixed, load.reshape(n)


def solution(mesh):
    placed = (
        P(("ep", "tp"), None),
        P(),
        P(("ep", "tp"), None),
        P(("ep", "tp"), None),
        P("tp", None, None),
        P("tp", None, None),
        P("tp", None, None),
        P(),
        P(),
        P(),
    )
    return jax.shard_map(
        per_device,
        mesh=mesh,
        in_specs=placed,
        out_specs=(P(("ep", "tp"), None), P()),
        check_vma=False,
    )
```

```python
import functools

import jax
import jax.numpy as jnp
from jax import lax
from jax.experimental import pallas as pl
from jax.experimental.pallas import tpu as pltpu
from jax.sharding import PartitionSpec as P

F32 = jnp.float32
BF16 = jnp.bfloat16


def direct(
    n,
    eps,
    cap,
    tokens_hbm,
    routes,
    gates,
    gain,
    expert_gate,
    expert_up,
    expert_down,
    shared_gate,
    shared_up,
    shared_down,
    out,
    load,
    tokens,
    blocks,
    group_routes,
    every_routes,
    rows_in,
    hidden,
    results,
    returned,
    total,
    w_gate,
    w_up,
    w_down,
    s_gate,
    s_up,
    s_down,
    weight_sem,
    own_sem,
    route_send,
    route_recv,
    far_send,
    far_recv,
    token_send,
    token_recv,
    result_send,
    result_recv,
):
    me = lax.axis_index("tp")
    here = lax.axis_index("ep")
    rows, width = tokens.shape
    half = rows // 2
    chunk = rows // cap
    order = [lax.rem(me + i, n) for i in range(n)]

    barrier = pltpu.get_barrier_semaphore()
    planes = [lax.rem(here + i, eps) for i in range(1, eps)]
    for peer in order[1:]:
        pl.semaphore_signal(barrier, inc=1, device_id={"tp": peer})
    for plane in planes:
        pl.semaphore_signal(barrier, inc=1, device_id={"ep": plane})
    own_tokens = pltpu.make_async_copy(tokens_hbm, tokens, own_sem.at[1])
    own_tokens.start()

    weights = [
        pltpu.make_async_copy(src, dst, weight_sem.at[i])
        for i, (src, dst) in enumerate(
            [
                (expert_gate.at[0], w_gate),
                (expert_up.at[0], w_up),
                (expert_down.at[0], w_down),
                (shared_gate, s_gate),
                (shared_up, s_up),
                (shared_down, s_down),
            ]
        )
    ]
    for copy in weights:
        copy.start()
    own_routes = pltpu.make_async_copy(routes, group_routes.at[me], own_sem.at[0])
    own_routes.start()

    pl.semaphore_wait(barrier, n - 1 + eps - 1)

    pending = []
    for i, peer in enumerate(order[1:]):
        copy = pltpu.make_async_remote_copy(
            src_ref=routes,
            dst_ref=group_routes.at[me],
            send_sem=route_send.at[i],
            recv_sem=route_recv.at[me],
            device_id={"tp": peer},
        )
        copy.start()
        pending.append(copy)

    def part(ref, piece):
        return ref.at[pl.ds(piece * half, half)]

    def send(source, piece, slot, peer, number):
        copy = pltpu.make_async_remote_copy(
            src_ref=part(source, piece),
            dst_ref=part(blocks.at[slot], piece),
            send_sem=token_send.at[number],
            recv_sem=token_recv.at[slot, piece],
            device_id={"tp": peer},
        )
        copy.start()
        pending.append(copy)

    def landed(slot, piece):
        ref = part(blocks.at[slot], piece)
        pltpu.make_async_copy(ref, ref, token_recv.at[slot, piece]).wait()

    own_tokens.wait()
    for i, peer in enumerate(order[1:]):
        send(tokens, 0, me, peer, 2 * i)
        send(tokens, 1, me, peer, 2 * i + 1)

    earlier = (
        lax.broadcasted_iota(jnp.int32, (rows, rows), 0)
        < lax.broadcasted_iota(jnp.int32, (rows, rows), 1)
    ).astype(BF16)
    row_in_slot = lax.broadcasted_iota(jnp.int32, (cap, rows), 0)

    def normed_of(values):
        center = jnp.mean(values, axis=-1, keepdims=True)
        values = values - center
        spread = jnp.mean(jnp.square(values), axis=-1, keepdims=True)
        return (values * lax.rsqrt(spread + 1e-05) * gain[...]).astype(BF16)

    def gated(values, gate_ref, up_ref):
        gate_part = jnp.dot(values, gate_ref[...], preferred_element_type=F32)
        up_part = jnp.dot(values, up_ref[...], preferred_element_type=F32)
        return (gate_part * (1.0 / (1.0 + jnp.exp(-gate_part))) * up_part).astype(BF16)

    def gather(i, at):
        source = order[i]
        named = group_routes[source]
        member = (named[0:1] == me) | (named[1:2] == me)
        count = jnp.dot(
            jnp.broadcast_to(member.astype(F32), (8, rows)).astype(BF16),
            earlier,
            preferred_element_type=F32,
        )[0:1].astype(jnp.int32)
        slot = jnp.where(member, count, -1)
        pick = (row_in_slot == slot).astype(F32).astype(BF16)
        held = tokens[...] if i == 0 else blocks[source]
        taken = jnp.dot(pick, held, preferred_element_type=F32)
        rows_in[at * cap : (at + 1) * cap, :] = normed_of(taken)

    tile = 512

    def expert(members):
        count = len(members) * cap
        hidden[:count] = gated(rows_in[:count], w_gate, w_up)
        for at in range(0, width, tile):
            value = jnp.dot(
                hidden[:count], w_down[:, at : at + tile], preferred_element_type=F32
            ).astype(BF16)
            for g, i in enumerate(members):
                piece = value[g * cap : (g + 1) * cap]
                if i == 0:
                    returned[me, :, at : at + tile] = piece
                else:
                    results[i, :, at : at + tile] = piece
        for i in members:
            if i == 0:
                continue
            copy = pltpu.make_async_remote_copy(
                src_ref=results.at[i],
                dst_ref=returned.at[me],
                send_sem=result_send.at[i],
                recv_sem=result_recv.at[me],
                device_id={"tp": order[i]},
            )
            copy.start()
            pending.append(copy)

    own_routes.wait()
    for peer in order[1:]:
        ref = group_routes.at[peer]
        pltpu.make_async_copy(ref, ref, route_recv.at[peer]).wait()
    for i, plane in enumerate(planes):
        copy = pltpu.make_async_remote_copy(
            src_ref=group_routes,
            dst_ref=every_routes.at[here],
            send_sem=far_send.at[i],
            recv_sem=far_recv.at[here],
            device_id={"ep": plane},
        )
        copy.start()
        pending.append(copy)

    for copy in weights[:3]:
        copy.wait()
    for number in range(n // chunk):
        members = list(range(number * chunk, (number + 1) * chunk))
        for i in members:
            if i > 0:
                landed(order[i], 0)
                landed(order[i], 1)
            gather(i, i % chunk)
        expert(members)

    for copy in weights[3:]:
        copy.wait()
    rows_in[:rows] = normed_of(tokens[...].astype(F32))
    shared = gated(rows_in[:rows], s_gate, s_up)
    for at in range(0, width, tile):
        total[:, at : at + tile] = jnp.dot(
            shared, s_down[:, at : at + tile], preferred_element_type=F32
        )

    expert_ids = lax.broadcasted_iota(jnp.int32, (n, rows), 0)
    first, second = routes[0:1], routes[1:2]
    member = ((first == expert_ids) | (second == expert_ids)).astype(F32)
    ranks = jnp.dot(member.astype(BF16), earlier, preferred_element_type=F32)
    slots = [
        named * cap
        + jnp.sum(jnp.where(named == expert_ids, ranks, 0.0), axis=0, keepdims=True).astype(jnp.int32)
        for named in (first, second)
    ]

    def counted(ref_of, amount, start):
        def step(i, sums):
            named = ref_of(i)
            return (
                sums
                + (named[0:1] == expert_ids).astype(F32)
                + (named[1:2] == expert_ids).astype(F32)
            )

        return lax.fori_loop(0, amount, step, start)

    sums = counted(lambda i: group_routes[i], n, jnp.zeros((n, rows), F32))
    for plane in planes:
        ref = every_routes.at[plane]
        pltpu.make_async_copy(ref, ref, far_recv.at[plane]).wait()
        sums = counted(lambda i, plane=plane: every_routes[plane, i], n, sums)
    counts = lax.dot_general(
        jnp.ones((8, rows), F32),
        sums,
        (((1,), (1,)), ((), ())),
        precision=lax.Precision.HIGHEST,
        preferred_element_type=F32,
    )
    load[...] = counts[0:1, :] * (n / (rows * 2 * n * eps))

    columns = jnp.transpose(jnp.broadcast_to(gates[0:1], (8, rows))), jnp.transpose(
        jnp.broadcast_to(gates[1:2], (8, rows))
    )
    gate_of = [column[:, 0:1] for column in columns]
    parts = [list(range(at, at + chunk)) for at in range(0, n, chunk)]
    for members in parts:
        sources = [order[i] for i in members]
        picks = [
            jnp.transpose(
                jnp.concatenate(
                    [(row_in_slot + source * cap == slot).astype(F32) for source in sources], axis=0
                )
            ).astype(BF16)
            for slot in slots
        ]
        for i, source in zip(members, sources):
            if i > 0:
                ref = returned.at[source]
                pltpu.make_async_copy(ref, ref, result_recv.at[source]).wait()
        last = members is parts[-1]
        for at in range(0, width, tile):
            back = jnp.concatenate([returned[source, :, at : at + tile] for source in sources], axis=0)
            value = total[:, at : at + tile]
            for k in range(2):
                value = value + gate_of[k] * jnp.dot(picks[k], back, preferred_element_type=F32)
            if last:
                out[:, at : at + tile] = value.astype(BF16)
            else:
                total[:, at : at + tile] = value

    for copy in pending:
        copy.wait_send()


def square(
    eps,
    tokens_hbm,
    routes_hbm,
    gates_hbm,
    gain_hbm,
    expert_gate,
    expert_up,
    expert_down,
    shared_gate,
    shared_up,
    shared_down,
    out,
    load,
    blocks,
    routes,
    gates,
    gain,
    near_routes,
    near_gates,
    tally,
    lanes,
    columns,
    normed,
    hidden,
    mine,
    lent,
    theirs,
    shared,
    merged,
    passed,
    back,
    base,
    w_in,
    w_down,
    s_in,
    s_down,
    sems,
    entered,
    meta_recv,
    tally_recv,
    token_recv,
    core_recv,
    result_recv,
    passed_recv,
    back_recv,
):
    n = 8
    me = lax.axis_index("tp")
    here = lax.axis_index("ep")
    rows, width = out.shape
    half, quarter = rows // 2, rows // 4
    piece = 16
    steps = half // piece
    core, xbit, ybit = me % 2, (me // 2) % 2, me // 4
    across = 1 - 2 * core
    sib = me + across
    nx = me + 2 * (1 - 2 * xbit)
    ny = me + 4 * (1 - 2 * ybit)
    nd = nx + 4 * (1 - 2 * ybit)
    column_head = me == 0
    below, above = column_head & (here > 0), column_head & (here < eps - 1)

    copies = [
        (2, routes_hbm, routes),
        (2, gates_hbm, gates),
        (0, tokens_hbm.at[pl.ds(0, half)], blocks.at[0, pl.ds(0, half)]),
        (1, tokens_hbm.at[pl.ds(half, half)], blocks.at[0, pl.ds(half, half)]),
        (3, gain_hbm, gain),
        (4, expert_gate.at[0], w_in.at[0]),
        (4, expert_up.at[0], w_in.at[1]),
        (5, expert_down.at[0], w_down),
        (6, shared_gate, s_in.at[0]),
        (6, shared_up, s_in.at[1]),
        (7, shared_down, s_down),
    ]
    for number, source, target in copies[:4]:
        pltpu.make_async_copy(source, target, sems.at[number]).start()

    barrier = pltpu.get_barrier_semaphore()
    edges = [(core, sib), (xbit, nx), (ybit, ny)]
    for bit, peer in edges:

        @pl.when(bit == 0)
        def _():
            pl.semaphore_signal(barrier, inc=1, device_id={"tp": peer})

    @pl.when(above)
    def _():
        pl.semaphore_signal(barrier, inc=1, device_id={"ep": here + 1})

    for number, source, target in copies[4:]:
        pltpu.make_async_copy(source, target, sems.at[number]).start()

    def arrived(ref, sem):
        pltpu.make_async_copy(ref, ref, sem).wait()


    @pl.when(me + here > 0)
    def _():
        pl.semaphore_wait(barrier, core + xbit + ybit + jnp.where(below, 1, 0))

    for number, (bit, peer) in enumerate(edges):

        @pl.when(bit == 1)
        def _():
            pl.semaphore_signal(entered.at[number], inc=1, device_id={"tp": peer})

    @pl.when(below)
    def _():
        pl.semaphore_signal(entered.at[3], inc=1, device_id={"ep": here - 1})

    def send(source, target, send_sem, recv_sem, where):
        pltpu.make_async_remote_copy(
            src_ref=source,
            dst_ref=target,
            send_sem=send_sem,
            recv_sem=recv_sem,
            device_id=where,
        ).start()

    def at_rows(ref, start, size):
        return ref.at[pl.ds(start, size)]

    def link(source, target, start, size, recv_sem, peer):
        send(
            at_rows(source, start, size),
            at_rows(target, start, size),
            sems.at[0],
            recv_sem,
            {"tp": peer},
        )

    def token_send(source, start, size, group, number, peer):
        link(blocks.at[source], blocks.at[group], start, size, token_recv.at[number], peer)

    def lend(group, start, size):
        send(
            at_rows(blocks.at[group], start, size),
            at_rows(blocks.at[group + 4], start, size),
            sems.at[1],
            core_recv.at[group],
            {"tp": sib},
        )

    def landed(group, start, size, number):
        arrived(at_rows(blocks.at[group], start, size), token_recv.at[number])

    def introduce(i):
        peer = (nx, ny)[i]
        send(routes, near_routes.at[i], sems.at[2], meta_recv.at[0], {"tp": peer})
        send(gates, near_gates.at[i], sems.at[2], meta_recv.at[0], {"tp": peer})

    def open_link(i):
        token_send(0, i * half, half, 1, i, (nx, ny)[i])

    arrived(at_rows(near_routes, 0, 2), sems.at[2])
    for i in range(2):

        @pl.when(edges[1 + i][0] == 1)
        def _():
            introduce(i)

    for i in range(2):
        arrived(blocks.at[0, pl.ds(i * half, half)], sems.at[i])

        @pl.when(edges[1 + i][0] == 1)
        def _():
            open_link(i)

    @pl.when(core == 0)
    def _():
        pl.semaphore_wait(entered.at[0], 1)

    lend(0, 0, rows)
    for i in range(2):

        @pl.when(edges[1 + i][0] == 0)
        def _():
            pl.semaphore_wait(entered.at[1 + i], 1)
            introduce(i)
            open_link(i)

    expert_ids = lax.broadcasted_iota(jnp.int32, (n, rows), 0)

    def tallied(route):
        return (route[0:1] == expert_ids).astype(F32) + (route[1:2] == expert_ids).astype(F32)

    def tally_send(source, target, number, recv, where):
        send(tally.at[source], tally.at[target], sems.at[number], tally_recv.at[recv], where)

    def along_column(rounds):
        for r in rounds:

            @pl.when(column_head & (here == r))
            def _():
                value = tally[2]
                if r > 0:
                    arrived(tally.at[3], tally_recv.at[1])
                    value = value + tally[3]
                tally[5] = value
                if r < eps - 1:
                    tally_send(5, 3, 3, 1, {"ep": here + 1})

            @pl.when(column_head & (here == eps - 1 - r))
            def _():
                value = tally[2]
                if r > 0:
                    arrived(tally.at[4], tally_recv.at[2])
                    value = value + tally[4]
                tally[6] = value
                if r < eps - 1:
                    tally_send(6, 4, 4, 2, {"ep": here - 1})

    handers = [
        (column_head, (sib, nx, ny)),
        ((core == 0) & (xbit == 1) & (ybit == 0), (sib, ny)),
        ((core == 0) & (xbit == 0) & (ybit == 1), (sib,)),
        ((core == 0) & (xbit == 1) & (ybit == 1), (sib,)),
        (core == 1, ()),
    ]

    def hand_on(number):
        test, peers = handers[number]

        @pl.when(test)
        def _():
            if number > 0:
                arrived(tally.at[7], tally_recv.at[3])
            for peer in peers:
                tally_send(7, 7, 2, 3, {"tp": peer})

    def norm(group, slot=0):
        values = blocks[group].astype(F32)
        center = jnp.mean(values, axis=-1, keepdims=True)
        values = values - center
        spread = jnp.mean(jnp.square(values), axis=-1, keepdims=True)
        normed[slot] = (values * lax.rsqrt(spread + 1e-05) * gain[...]).astype(BF16)

    def gated(values, gate_ref, up_ref):
        gate_part = jnp.dot(values, gate_ref[...], preferred_element_type=F32)
        up_part = jnp.dot(values, up_ref[...], preferred_element_type=F32)
        return (gate_part * (1.0 / (1.0 + jnp.exp(-gate_part))) * up_part).astype(BF16)

    tile = 512

    def expert(result, slot=0):
        hidden[...] = gated(normed[slot], w_in.at[0], w_in.at[1])
        for at in range(0, width, tile):
            result[:, at : at + tile] = jnp.dot(
                hidden[...], w_down[:, at : at + tile], preferred_element_type=F32
            ).astype(BF16)

    def common(group):
        inner = gated(normed[0], s_in.at[0], s_in.at[1])
        for at in range(0, width, tile):
            shared[group, :, at : at + tile] = jnp.dot(
                inner, s_down[:, at : at + tile], preferred_element_type=F32
            )

    def serve(group):
        arrived(blocks.at[group + 4], core_recv.at[group])
        norm(group + 4, 1)
        expert(lent.at[group], 1)
        send(lent.at[group], theirs.at[group], sems.at[1], result_recv.at[group], {"tp": sib})

    def named(ids):
        def test(route):
            hit = route == ids[0]
            for one in ids[1:]:
                hit = hit | (route == one)
            return hit

        return test

    def share(route, gate, test):
        first, second = test(route[0:1]), test(route[1:2])
        amount = first.astype(F32) + second.astype(F32)
        weight = jnp.where(first, gate[0:1], jnp.where(second, gate[1:2], 0.0))
        return amount, weight

    def store_columns(group, values):
        for i, value in enumerate(values):
            lanes[group, i : i + 1] = value
        columns[group] = jnp.transpose(lanes[group])

    lane = lax.broadcasted_iota(jnp.int32, (2, rows), 1)
    low = lane < half
    low_row = low[0:1]
    is_me, is_sib = named([me]), named([sib])
    on_x, on_y = named([nx, nx + across]), named([ny, ny + across])
    on_xd = named([nx, nx + across, nd, nd + across])
    on_yd = named([ny, ny + across, nd, nd + across])

    def coefficients(group, route, gate, relayed=False):
        mine_n, mine_g = share(route, gate, is_me)
        sib_n, sib_g = share(route, gate, is_sib)
        both = mine_n + sib_n
        if relayed:
            by_x, by_y = share(route, gate, on_x), share(route, gate, on_y)
            far_n, far_g = [jnp.where(low_row, a, b) for a, b in zip(by_x, by_y)]
            full = (both + far_n == 2.0) & (far_n < 2.0)
        else:
            full = both == 2.0
        values = [
            jnp.where(full, mine_g, mine_n),
            jnp.where(full, sib_g, sib_n),
            full.astype(F32),
        ]
        if relayed:
            values.append(jnp.where(full, far_g, 1.0))
        store_columns(group, values)

    def own_coefficients():
        route, gate = routes[...], gates[...]
        _, mine_g = share(route, gate, is_me)
        _, sib_g = share(route, gate, is_sib)
        x_low, x_high = share(route, gate, on_x), share(route, gate, on_xd)
        y_low, y_high = share(route, gate, on_yd), share(route, gate, on_y)
        x_n, x_g = [jnp.where(low_row, a, b) for a, b in zip(x_low, x_high)]
        y_n, y_g = [jnp.where(low_row, a, b) for a, b in zip(y_low, y_high)]
        done_x, done_y = x_n == 2.0, y_n == 2.0
        store_columns(
            0,
            [
                mine_g,
                sib_g,
                jnp.where(done_x | done_y, 0.0, 1.0),
                jnp.where(done_x, 1.0, x_g),
                jnp.where(done_y, 1.0, y_g),
            ],
        )

    def column(group, i, start, size):
        return columns[group, pl.ds(start, size), i : i + 1]

    def local_sum(group, start, size):
        where = pl.ds(start, size)
        return (
            column(group, 0, start, size) * mine[group, where].astype(F32)
            + column(group, 1, start, size) * theirs[group, where].astype(F32)
            + column(group, 2, start, size) * shared[group, where]
        )

    def into_sum(total, group):
        def step(i, carry):
            start = pl.multiple_of(i * piece, piece)
            total[pl.ds(start, piece)] = local_sum(group, start, piece)
            return carry

        lax.fori_loop(0, rows // piece, step, 0)

    def merge(group, target_of, recv_of):
        for step in range(steps):
            for first, peer in ((0, nx), (1, ny)):
                start = first * half + step * piece
                merged[group, pl.ds(start, piece)] = local_sum(group, start, piece).astype(BF16)
                link(merged.at[group], target_of(first), start, piece, recv_of(step), peer)

    arrived(gain, sems.at[3])
    norm(0)
    arrived(w_in, sems.at[4])
    arrived(w_down, sems.at[5])
    expert(mine.at[0])
    arrived(s_in, sems.at[6])
    arrived(s_down, sems.at[7])
    common(0)
    serve(0)

    arrived(tally.at[0], meta_recv.at[0])
    arrived(tally.at[0], sems.at[2])
    send(near_routes.at[0], near_routes.at[2], sems.at[2], meta_recv.at[1], {"tp": ny})
    send(near_gates.at[0], near_gates.at[2], sems.at[2], meta_recv.at[1], {"tp": ny})
    token_send(0, half, quarter, 2, 2, nx)
    token_send(0, 0, quarter, 2, 2, ny)
    own_coefficients()
    x_route, y_route = near_routes[0], near_routes[1]
    x_gate, y_gate = near_gates[0], near_gates[1]
    coefficients(1, jnp.where(low, x_route, y_route), jnp.where(low, x_gate, y_gate))
    coefficients(
        2,
        jnp.where(low, y_route, x_route),
        jnp.where(low, y_gate, x_gate),
        relayed=True,
    )

    landed(1, 0, half, 0)
    token_send(1, 0, quarter, 3, 4, ny)
    token_send(1, quarter, quarter, 3, 5, ny)
    lend(1, 0, half)
    landed(1, half, half, 1)
    token_send(1, half, quarter, 3, 4, nx)
    token_send(1, half + quarter, quarter, 3, 5, nx)
    lend(1, half, half)
    token_send(0, half + quarter, quarter, 2, 3, nx)
    token_send(0, quarter, quarter, 2, 3, ny)
    arrived(at_rows(near_routes, 0, 2), meta_recv.at[1])
    d_route = near_routes[2]
    tally[0] = tallied(routes[...]) + tallied(x_route) + tallied(y_route) + tallied(d_route)
    arrived(at_rows(near_routes, 0, 2), sems.at[2])
    tally_send(0, 1, 2, 0, {"tp": sib})
    norm(1)
    expert(mine.at[1])
    arrived(tally.at[1], tally_recv.at[0])
    arrived(tally.at[0], sems.at[2])
    tally[2] = tally[0] + tally[1]
    rounds = list(range(eps))

    @pl.when(above)
    def _():
        pl.semaphore_wait(entered.at[3], 1)

    along_column(rounds[:1])
    serve(1)
    common(1)
    coefficients(3, d_route, near_gates[2])
    arrived(theirs.at[0], result_recv.at[0])
    into_sum(base, 0)
    landed(2, 0, half, 2)
    lend(2, half, quarter)
    lend(2, 0, quarter)
    along_column(rounds[1:2])
    arrived(theirs.at[1], result_recv.at[1])
    merge(1, lambda first: back.at[first], lambda step: back_recv.at[steps])

    landed(3, 0, half, 4)
    lend(3, 0, quarter)
    lend(3, half, quarter)
    landed(3, 0, half, 5)
    lend(3, quarter, quarter)
    lend(3, half + quarter, quarter)
    along_column(rounds[2:3])
    norm(3)
    common(3)
    serve(3)
    expert(mine.at[3])
    landed(2, 0, half, 3)
    lend(2, half + quarter, quarter)
    lend(2, quarter, quarter)
    along_column(rounds[3:])

    @pl.when(column_head)
    def _():
        tally[7] = tally[5] + tally[6] - tally[2]

    hand_on(0)
    arrived(theirs.at[3], result_recv.at[3])
    merge(3, lambda first: passed, lambda step: passed_recv.at[step])
    serve(2)
    norm(2)
    expert(mine.at[2])
    common(2)
    arrived(theirs.at[2], result_recv.at[2])
    into_sum(shared.at[2], 2)
    hand_on(1)
    hand_on(2)

    for step in range(steps):
        arrived(at_rows(passed, 0, 2 * piece), passed_recv.at[step])
        for first, peer in ((1, nx), (0, ny)):
            start = first * half + step * piece
            where = pl.ds(start, piece)
            merged[2, where] = (
                shared[2, where] + column(2, 3, start, piece) * passed[where].astype(F32)
            ).astype(BF16)
            link(merged.at[2], back.at[1 - first], start, piece, back_recv.at[step], peer)

    arrived(at_rows(back.at[0], 0, rows), back_recv.at[steps])

    def early(i, carry):
        for first in range(2):
            start = pl.multiple_of(first * half + i * piece, piece)
            where = pl.ds(start, piece)
            base[where] = base[where] + column(0, 3 + first, start, piece) * back[
                first, where
            ].astype(F32)
        return carry

    lax.fori_loop(0, steps, early, 0)

    hand_on(3)
    hand_on(4)
    counts = lax.dot_general(
        jnp.ones((8, rows), F32),
        tally[7],
        (((1,), (1,)), ((), ())),
        precision=lax.Precision.HIGHEST,
        preferred_element_type=F32,
    )
    load[...] = counts[0:1, :] * (n / (rows * 2 * n * eps))

    for step in range(steps):
        arrived(at_rows(back.at[0], 0, 2 * piece), back_recv.at[step])
        for first in range(2):
            start = (1 - first) * half + step * piece
            where = pl.ds(start, piece)
            out[where] = (
                base[where] + column(0, 3 + first, start, piece) * back[first, where].astype(F32)
            ).astype(BF16)

    arrived(at_rows(blocks, 0, 6), sems.at[0])
    arrived(blocks, sems.at[1])
    for number, test in ((3, above), (4, below)):

        @pl.when(test)
        def _():
            arrived(tally.at[0], sems.at[number])

    for test, peers in handers[:-1]:

        @pl.when(test)
        def _():
            arrived(at_rows(tally, 0, len(peers)), sems.at[2])


def write_out(mixed, load, mixed_out, load_out, sem):
    copies = [
        pltpu.make_async_copy(mixed, mixed_out, sem.at[0]),
        pltpu.make_async_copy(load, load_out, sem.at[1]),
    ]
    for copy in copies:
        copy.start()
    for copy in copies:
        copy.wait()


def per_device(
    tokens,
    norm_gain,
    routes,
    gates,
    expert_gate,
    expert_up,
    expert_down,
    shared_gate,
    shared_up,
    shared_down,
):
    n, eps = lax.axis_size("tp"), lax.axis_size("ep")
    rows, width = tokens.shape
    top = routes.shape[1]
    cap = 2 * rows * top // n
    units = expert_gate.shape[2]
    vmem = pl.BlockSpec(memory_space=pltpu.VMEM)
    hbm = pl.BlockSpec(memory_space=pl.ANY)
    dma = pltpu.SemaphoreType.DMA
    if n == 8 and top == 2:
        body = functools.partial(square, eps)
        small = hbm
        scratch = [
            pltpu.VMEM((8, rows, width), BF16),
            pltpu.VMEM((top, rows), jnp.int32),
            pltpu.VMEM((top, rows), F32),
            pltpu.VMEM((1, width), F32),
            pltpu.VMEM((3, top, rows), jnp.int32),
            pltpu.VMEM((3, top, rows), F32),
            pltpu.VMEM((8, n, rows), F32),
            pltpu.VMEM((4, 8, rows), F32),
            pltpu.VMEM((4, rows, 8), F32),
            pltpu.VMEM((2, rows, width), BF16),
            pltpu.VMEM((rows, units), BF16),
            pltpu.VMEM((4, rows, width), BF16),
            pltpu.VMEM((4, rows, width), BF16),
            pltpu.VMEM((4, rows, width), BF16),
            pltpu.VMEM((4, rows, width), F32),
            pltpu.VMEM((4, rows, width), BF16),
            pltpu.VMEM((rows, width), BF16),
            pltpu.VMEM((2, rows, width), BF16),
            pltpu.VMEM((rows, width), F32),
            pltpu.VMEM((2, *expert_gate.shape[1:]), BF16),
            pltpu.VMEM(expert_down.shape[1:], BF16),
            pltpu.VMEM((2, *shared_gate.shape), BF16),
            pltpu.VMEM(shared_down.shape, BF16),
            dma((8,)),
            pltpu.SemaphoreType.REGULAR((4,)),
            dma((2,)),
            dma((4,)),
            dma((6,)),
            dma((4,)),
            dma((4,)),
            dma((rows // 32,)),
            dma((rows // 32 + 1,)),
        ]
    else:
        body = functools.partial(direct, n, eps, cap)
        small = vmem
        scratch = [
            pltpu.VMEM((rows, width), BF16),
            pltpu.VMEM((n, rows, width), BF16),
            pltpu.VMEM((n, top, rows), jnp.int32),
            pltpu.VMEM((eps, n, top, rows), jnp.int32),
            pltpu.VMEM((rows, width), BF16),
            pltpu.VMEM((rows, units), BF16),
            pltpu.VMEM((n, cap, width), BF16),
            pltpu.VMEM((n, cap, width), BF16),
            pltpu.VMEM((rows, width), F32),
            pltpu.VMEM(expert_gate.shape[1:], BF16),
            pltpu.VMEM(expert_up.shape[1:], BF16),
            pltpu.VMEM(expert_down.shape[1:], BF16),
            pltpu.VMEM(shared_gate.shape, BF16),
            pltpu.VMEM(shared_up.shape, BF16),
            pltpu.VMEM(shared_down.shape, BF16),
            dma((6,)),
            dma((2,)),
            dma((n - 1,)),
            dma((n,)),
            dma((max(1, eps - 1),)),
            dma((eps,)),
            dma((2 * (n - 1),)),
            dma((n, 2)),
            dma((n,)),
            dma((n,)),
        ]
    mixed, load = pl.pallas_call(
        body,
        out_shape=(
            pltpu.VMEM((rows, width), BF16),
            pltpu.VMEM((1, n), F32),
        ),
        in_specs=[hbm] + [small] * 3 + [hbm] * 6,
        out_specs=(vmem, vmem),
        scratch_shapes=scratch,
        compiler_params=pltpu.CompilerParams(
            collective_id=0, has_side_effects=True
        ),
    )(
        tokens,
        routes.T,
        gates.T,
        norm_gain.reshape(1, width),
        expert_gate,
        expert_up,
        expert_down,
        shared_gate,
        shared_up,
        shared_down,
    )
    mixed, load = pl.pallas_call(
        write_out,
        out_shape=(
            jax.ShapeDtypeStruct((rows, width), BF16),
            jax.ShapeDtypeStruct((1, n), F32),
        ),
        in_specs=[vmem] * 2,
        out_specs=(hbm, hbm),
        scratch_shapes=[dma((2,))],
        compiler_params=pltpu.CompilerParams(vmem_limit_bytes=1 << 20),
    )(mixed, load)
    return mixed, load.reshape(n)


def solution(mesh):
    placed = (
        P(("ep", "tp"), None),
        P(),
        P(("ep", "tp"), None),
        P(("ep", "tp"), None),
        P("tp", None, None),
        P("tp", None, None),
        P("tp", None, None),
        P(),
        P(),
        P(),
    )
    return jax.shard_map(
        per_device,
        mesh=mesh,
        in_specs=placed,
        out_specs=(P(("ep", "tp"), None), P()),
        check_vma=False,
    )
```

```python
import functools

import jax
import jax.numpy as jnp
from jax import lax
from jax.experimental import pallas as pl
from jax.experimental.pallas import tpu as pltpu
from jax.sharding import PartitionSpec as P

F32 = jnp.float32
BF16 = jnp.bfloat16


def direct(
    n,
    eps,
    cap,
    tokens_hbm,
    routes,
    gates,
    gain,
    expert_gate,
    expert_up,
    expert_down,
    shared_gate,
    shared_up,
    shared_down,
    out,
    load,
    tokens,
    blocks,
    group_routes,
    every_routes,
    rows_in,
    hidden,
    results,
    returned,
    total,
    w_gate,
    w_up,
    w_down,
    s_gate,
    s_up,
    s_down,
    weight_sem,
    own_sem,
    route_send,
    route_recv,
    far_send,
    far_recv,
    token_send,
    token_recv,
    result_send,
    result_recv,
):
    me = lax.axis_index("tp")
    here = lax.axis_index("ep")
    rows, width = tokens.shape
    half = rows // 2
    chunk = rows // cap
    order = [lax.rem(me + i, n) for i in range(n)]

    barrier = pltpu.get_barrier_semaphore()
    planes = [lax.rem(here + i, eps) for i in range(1, eps)]
    for peer in order[1:]:
        pl.semaphore_signal(barrier, inc=1, device_id={"tp": peer})
    for plane in planes:
        pl.semaphore_signal(barrier, inc=1, device_id={"ep": plane})
    own_tokens = pltpu.make_async_copy(tokens_hbm, tokens, own_sem.at[1])
    own_tokens.start()

    weights = [
        pltpu.make_async_copy(src, dst, weight_sem.at[i])
        for i, (src, dst) in enumerate(
            [
                (expert_gate.at[0], w_gate),
                (expert_up.at[0], w_up),
                (expert_down.at[0], w_down),
                (shared_gate, s_gate),
                (shared_up, s_up),
                (shared_down, s_down),
            ]
        )
    ]
    for copy in weights:
        copy.start()
    own_routes = pltpu.make_async_copy(routes, group_routes.at[me], own_sem.at[0])
    own_routes.start()

    pl.semaphore_wait(barrier, n - 1 + eps - 1)

    pending = []
    for i, peer in enumerate(order[1:]):
        copy = pltpu.make_async_remote_copy(
            src_ref=routes,
            dst_ref=group_routes.at[me],
            send_sem=route_send.at[i],
            recv_sem=route_recv.at[me],
            device_id={"tp": peer},
        )
        copy.start()
        pending.append(copy)

    def part(ref, piece):
        return ref.at[pl.ds(piece * half, half)]

    def send(source, piece, slot, peer, number):
        copy = pltpu.make_async_remote_copy(
            src_ref=part(source, piece),
            dst_ref=part(blocks.at[slot], piece),
            send_sem=token_send.at[number],
            recv_sem=token_recv.at[slot, piece],
            device_id={"tp": peer},
        )
        copy.start()
        pending.append(copy)

    def landed(slot, piece):
        ref = part(blocks.at[slot], piece)
        pltpu.make_async_copy(ref, ref, token_recv.at[slot, piece]).wait()

    own_tokens.wait()
    for i, peer in enumerate(order[1:]):
        send(tokens, 0, me, peer, 2 * i)
        send(tokens, 1, me, peer, 2 * i + 1)

    earlier = (
        lax.broadcasted_iota(jnp.int32, (rows, rows), 0)
        < lax.broadcasted_iota(jnp.int32, (rows, rows), 1)
    ).astype(BF16)
    row_in_slot = lax.broadcasted_iota(jnp.int32, (cap, rows), 0)

    def normed_of(values):
        center = jnp.mean(values, axis=-1, keepdims=True)
        values = values - center
        spread = jnp.mean(jnp.square(values), axis=-1, keepdims=True)
        return (values * lax.rsqrt(spread + 1e-05) * gain[...]).astype(BF16)

    def gated(values, gate_ref, up_ref):
        gate_part = jnp.dot(values, gate_ref[...], preferred_element_type=F32)
        up_part = jnp.dot(values, up_ref[...], preferred_element_type=F32)
        return (gate_part * (1.0 / (1.0 + jnp.exp(-gate_part))) * up_part).astype(BF16)

    def gather(i, at):
        source = order[i]
        named = group_routes[source]
        member = (named[0:1] == me) | (named[1:2] == me)
        count = jnp.dot(
            jnp.broadcast_to(member.astype(F32), (8, rows)).astype(BF16),
            earlier,
            preferred_element_type=F32,
        )[0:1].astype(jnp.int32)
        slot = jnp.where(member, count, -1)
        pick = (row_in_slot == slot).astype(F32).astype(BF16)
        held = tokens[...] if i == 0 else blocks[source]
        taken = jnp.dot(pick, held, preferred_element_type=F32)
        rows_in[at * cap : (at + 1) * cap, :] = normed_of(taken)

    tile = 512

    def expert(members):
        count = len(members) * cap
        hidden[:count] = gated(rows_in[:count], w_gate, w_up)
        for at in range(0, width, tile):
            value = jnp.dot(
                hidden[:count], w_down[:, at : at + tile], preferred_element_type=F32
            ).astype(BF16)
            for g, i in enumerate(members):
                piece = value[g * cap : (g + 1) * cap]
                if i == 0:
                    returned[me, :, at : at + tile] = piece
                else:
                    results[i, :, at : at + tile] = piece
        for i in members:
            if i == 0:
                continue
            copy = pltpu.make_async_remote_copy(
                src_ref=results.at[i],
                dst_ref=returned.at[me],
                send_sem=result_send.at[i],
                recv_sem=result_recv.at[me],
                device_id={"tp": order[i]},
            )
            copy.start()
            pending.append(copy)

    own_routes.wait()
    for peer in order[1:]:
        ref = group_routes.at[peer]
        pltpu.make_async_copy(ref, ref, route_recv.at[peer]).wait()
    for i, plane in enumerate(planes):
        copy = pltpu.make_async_remote_copy(
            src_ref=group_routes,
            dst_ref=every_routes.at[here],
            send_sem=far_send.at[i],
            recv_sem=far_recv.at[here],
            device_id={"ep": plane},
        )
        copy.start()
        pending.append(copy)

    for copy in weights[:3]:
        copy.wait()
    for number in range(n // chunk):
        members = list(range(number * chunk, (number + 1) * chunk))
        for i in members:
            if i > 0:
                landed(order[i], 0)
                landed(order[i], 1)
            gather(i, i % chunk)
        expert(members)

    for copy in weights[3:]:
        copy.wait()
    rows_in[:rows] = normed_of(tokens[...].astype(F32))
    shared = gated(rows_in[:rows], s_gate, s_up)
    for at in range(0, width, tile):
        total[:, at : at + tile] = jnp.dot(
            shared, s_down[:, at : at + tile], preferred_element_type=F32
        )

    expert_ids = lax.broadcasted_iota(jnp.int32, (n, rows), 0)
    first, second = routes[0:1], routes[1:2]
    member = ((first == expert_ids) | (second == expert_ids)).astype(F32)
    ranks = jnp.dot(member.astype(BF16), earlier, preferred_element_type=F32)
    slots = [
        named * cap
        + jnp.sum(jnp.where(named == expert_ids, ranks, 0.0), axis=0, keepdims=True).astype(jnp.int32)
        for named in (first, second)
    ]

    def counted(ref_of, amount, start):
        def step(i, sums):
            named = ref_of(i)
            return (
                sums
                + (named[0:1] == expert_ids).astype(F32)
                + (named[1:2] == expert_ids).astype(F32)
            )

        return lax.fori_loop(0, amount, step, start)

    sums = counted(lambda i: group_routes[i], n, jnp.zeros((n, rows), F32))
    for plane in planes:
        ref = every_routes.at[plane]
        pltpu.make_async_copy(ref, ref, far_recv.at[plane]).wait()
        sums = counted(lambda i, plane=plane: every_routes[plane, i], n, sums)
    counts = lax.dot_general(
        jnp.ones((8, rows), F32),
        sums,
        (((1,), (1,)), ((), ())),
        precision=lax.Precision.HIGHEST,
        preferred_element_type=F32,
    )
    load[...] = counts[0:1, :] * (n / (rows * 2 * n * eps))

    columns = jnp.transpose(jnp.broadcast_to(gates[0:1], (8, rows))), jnp.transpose(
        jnp.broadcast_to(gates[1:2], (8, rows))
    )
    gate_of = [column[:, 0:1] for column in columns]
    parts = [list(range(at, at + chunk)) for at in range(0, n, chunk)]
    for members in parts:
        sources = [order[i] for i in members]
        picks = [
            jnp.transpose(
                jnp.concatenate(
                    [(row_in_slot + source * cap == slot).astype(F32) for source in sources], axis=0
                )
            ).astype(BF16)
            for slot in slots
        ]
        for i, source in zip(members, sources):
            if i > 0:
                ref = returned.at[source]
                pltpu.make_async_copy(ref, ref, result_recv.at[source]).wait()
        last = members is parts[-1]
        for at in range(0, width, tile):
            back = jnp.concatenate([returned[source, :, at : at + tile] for source in sources], axis=0)
            value = total[:, at : at + tile]
            for k in range(2):
                value = value + gate_of[k] * jnp.dot(picks[k], back, preferred_element_type=F32)
            if last:
                out[:, at : at + tile] = value.astype(BF16)
            else:
                total[:, at : at + tile] = value

    for copy in pending:
        copy.wait_send()


def square(
    eps,
    tokens_hbm,
    routes_hbm,
    gates_hbm,
    gain_hbm,
    expert_gate,
    expert_up,
    expert_down,
    shared_gate,
    shared_up,
    shared_down,
    out,
    load,
    blocks,
    routes,
    gates,
    gain,
    near_routes,
    near_gates,
    tally,
    lanes,
    columns,
    normed,
    hidden,
    mine,
    lent,
    theirs,
    shared,
    merged,
    passed,
    back,
    base,
    w_in,
    w_down,
    s_in,
    s_down,
    sems,
    entered,
    meta_recv,
    tally_recv,
    token_recv,
    core_recv,
    result_recv,
    passed_recv,
    back_recv,
):
    n = 8
    me = lax.axis_index("tp")
    here = lax.axis_index("ep")
    rows, width = out.shape
    half, quarter = rows // 2, rows // 4
    piece = 16
    steps = half // piece
    core, xbit, ybit = me % 2, (me // 2) % 2, me // 4
    across = 1 - 2 * core
    sib = me + across
    nx = me + 2 * (1 - 2 * xbit)
    ny = me + 4 * (1 - 2 * ybit)
    nd = nx + 4 * (1 - 2 * ybit)
    column_head = me == 0
    below, above = column_head & (here > 0), column_head & (here < eps - 1)

    copies = [
        (2, routes_hbm, routes),
        (2, gates_hbm, gates),
        (0, tokens_hbm.at[pl.ds(0, half)], blocks.at[0, pl.ds(0, half)]),
        (1, tokens_hbm.at[pl.ds(half, half)], blocks.at[0, pl.ds(half, half)]),
        (3, gain_hbm, gain),
        (4, expert_gate.at[0], w_in.at[0]),
        (4, expert_up.at[0], w_in.at[1]),
        (5, expert_down.at[0], w_down),
        (6, shared_gate, s_in.at[0]),
        (6, shared_up, s_in.at[1]),
        (7, shared_down, s_down),
    ]
    for number, source, target in copies[:4]:
        pltpu.make_async_copy(source, target, sems.at[number]).start()

    barrier = pltpu.get_barrier_semaphore()
    edges = [(core, sib), (xbit, nx), (ybit, ny)]
    for bit, peer in edges:

        @pl.when(bit == 0)
        def _():
            pl.semaphore_signal(barrier, inc=1, device_id={"tp": peer})

    @pl.when(above)
    def _():
        pl.semaphore_signal(barrier, inc=1, device_id={"ep": here + 1})

    for number, source, target in copies[4:]:
        pltpu.make_async_copy(source, target, sems.at[number]).start()

    def arrived(ref, sem):
        pltpu.make_async_copy(ref, ref, sem).wait()


    @pl.when(me + here > 0)
    def _():
        pl.semaphore_wait(barrier, core + xbit + ybit + jnp.where(below, 1, 0))

    for number, (bit, peer) in enumerate(edges):

        @pl.when(bit == 1)
        def _():
            pl.semaphore_signal(entered.at[number], inc=1, device_id={"tp": peer})

    @pl.when(below)
    def _():
        pl.semaphore_signal(entered.at[3], inc=1, device_id={"ep": here - 1})

    def send(source, target, send_sem, recv_sem, where):
        pltpu.make_async_remote_copy(
            src_ref=source,
            dst_ref=target,
            send_sem=send_sem,
            recv_sem=recv_sem,
            device_id=where,
        ).start()

    def at_rows(ref, start, size):
        return ref.at[pl.ds(start, size)]

    def link(source, target, start, size, recv_sem, peer):
        send(
            at_rows(source, start, size),
            at_rows(target, start, size),
            sems.at[0],
            recv_sem,
            {"tp": peer},
        )

    def token_send(source, start, size, group, number, peer):
        link(blocks.at[source], blocks.at[group], start, size, token_recv.at[number], peer)

    def lend(group, start, size):
        send(
            at_rows(blocks.at[group], start, size),
            at_rows(blocks.at[group + 4], start, size),
            sems.at[1],
            core_recv.at[group % 2],
            {"tp": sib},
        )

    def landed(group, start, size, number):
        arrived(at_rows(blocks.at[group], start, size), token_recv.at[number])

    def introduce(i):
        peer = (nx, ny)[i]
        send(routes, near_routes.at[i], sems.at[2], meta_recv.at[0], {"tp": peer})
        send(gates, near_gates.at[i], sems.at[2], meta_recv.at[0], {"tp": peer})

    def open_link(i):
        token_send(0, i * half, half, 1, i, (nx, ny)[i])

    arrived(at_rows(near_routes, 0, 2), sems.at[2])
    for i in range(2):

        @pl.when(edges[1 + i][0] == 1)
        def _():
            introduce(i)

    for i in range(2):
        arrived(blocks.at[0, pl.ds(i * half, half)], sems.at[i])

        @pl.when(edges[1 + i][0] == 1)
        def _():
            open_link(i)

    @pl.when(core == 0)
    def _():
        pl.semaphore_wait(entered.at[0], 1)

    lend(0, 0, rows)
    for i in range(2):

        @pl.when(edges[1 + i][0] == 0)
        def _():
            pl.semaphore_wait(entered.at[1 + i], 1)
            introduce(i)
            open_link(i)

    expert_ids = lax.broadcasted_iota(jnp.int32, (n, rows), 0)

    def tallied(route):
        return (route[0:1] == expert_ids).astype(F32) + (route[1:2] == expert_ids).astype(F32)

    def tally_send(source, target, number, recv, where):
        send(tally.at[source], tally.at[target], sems.at[number], tally_recv.at[recv], where)

    def along_column(rounds):
        for r in rounds:

            @pl.when(column_head & (here == r))
            def _():
                value = tally[2]
                if r > 0:
                    arrived(tally.at[3], tally_recv.at[1])
                    value = value + tally[3]
                tally[5] = value
                if r < eps - 1:
                    tally_send(5, 3, 3, 1, {"ep": here + 1})

            @pl.when(column_head & (here == eps - 1 - r))
            def _():
                value = tally[2]
                if r > 0:
                    arrived(tally.at[4], tally_recv.at[2])
                    value = value + tally[4]
                tally[6] = value
                if r < eps - 1:
                    tally_send(6, 4, 4, 2, {"ep": here - 1})

    handers = [
        (column_head, (sib, nx, ny)),
        ((core == 0) & (xbit == 1) & (ybit == 0), (sib, ny)),
        ((core == 0) & (xbit == 0) & (ybit == 1), (sib,)),
        ((core == 0) & (xbit == 1) & (ybit == 1), (sib,)),
        (core == 1, ()),
    ]

    def hand_on(number):
        test, peers = handers[number]

        @pl.when(test)
        def _():
            if number > 0:
                arrived(tally.at[7], tally_recv.at[3])
            for peer in peers:
                tally_send(7, 7, 2, 3, {"tp": peer})

    def norm(group, slot=0):
        values = blocks[group].astype(F32)
        center = jnp.mean(values, axis=-1, keepdims=True)
        values = values - center
        spread = jnp.mean(jnp.square(values), axis=-1, keepdims=True)
        normed[slot] = (values * lax.rsqrt(spread + 1e-05) * gain[...]).astype(BF16)

    def gated(values, gate_ref, up_ref):
        gate_part = jnp.dot(values, gate_ref[...], preferred_element_type=F32)
        up_part = jnp.dot(values, up_ref[...], preferred_element_type=F32)
        return (gate_part * (1.0 / (1.0 + jnp.exp(-gate_part))) * up_part).astype(BF16)

    tile = 512

    def expert(result, slot=0):
        hidden[...] = gated(normed[slot], w_in.at[0], w_in.at[1])
        for at in range(0, width, tile):
            result[:, at : at + tile] = jnp.dot(
                hidden[...], w_down[:, at : at + tile], preferred_element_type=F32
            ).astype(BF16)

    def common(group):
        inner = gated(normed[0], s_in.at[0], s_in.at[1])
        for at in range(0, width, tile):
            shared[group, :, at : at + tile] = jnp.dot(
                inner, s_down[:, at : at + tile], preferred_element_type=F32
            )

    def serve(group):
        arrived(blocks.at[group + 4], core_recv.at[group % 2])
        norm(group + 4, 1)
        expert(lent.at[group], 1)
        send(lent.at[group], theirs.at[group], sems.at[1], result_recv.at[group % 2], {"tp": sib})

    def named(ids):
        def test(route):
            hit = route == ids[0]
            for one in ids[1:]:
                hit = hit | (route == one)
            return hit

        return test

    def share(route, gate, test):
        first, second = test(route[0:1]), test(route[1:2])
        amount = first.astype(F32) + second.astype(F32)
        weight = jnp.where(first, gate[0:1], jnp.where(second, gate[1:2], 0.0))
        return amount, weight

    def store_columns(group, values):
        for i, value in enumerate(values):
            lanes[group, i : i + 1] = value
        columns[group] = jnp.transpose(lanes[group])

    lane = lax.broadcasted_iota(jnp.int32, (2, rows), 1)
    low = lane < half
    low_row = low[0:1]
    is_me, is_sib = named([me]), named([sib])
    on_x, on_y = named([nx, nx + across]), named([ny, ny + across])
    on_xd = named([nx, nx + across, nd, nd + across])
    on_yd = named([ny, ny + across, nd, nd + across])

    def coefficients(group, route, gate, relayed=False):
        mine_n, mine_g = share(route, gate, is_me)
        sib_n, sib_g = share(route, gate, is_sib)
        both = mine_n + sib_n
        if relayed:
            by_x, by_y = share(route, gate, on_x), share(route, gate, on_y)
            far_n, far_g = [jnp.where(low_row, a, b) for a, b in zip(by_x, by_y)]
            full = (both + far_n == 2.0) & (far_n < 2.0)
        else:
            full = both == 2.0
        values = [
            jnp.where(full, mine_g, mine_n),
            jnp.where(full, sib_g, sib_n),
            full.astype(F32),
        ]
        if relayed:
            values.append(jnp.where(full, far_g, 1.0))
        store_columns(group, values)

    def own_coefficients():
        route, gate = routes[...], gates[...]
        _, mine_g = share(route, gate, is_me)
        _, sib_g = share(route, gate, is_sib)
        x_low, x_high = share(route, gate, on_x), share(route, gate, on_xd)
        y_low, y_high = share(route, gate, on_yd), share(route, gate, on_y)
        x_n, x_g = [jnp.where(low_row, a, b) for a, b in zip(x_low, x_high)]
        y_n, y_g = [jnp.where(low_row, a, b) for a, b in zip(y_low, y_high)]
        done_x, done_y = x_n == 2.0, y_n == 2.0
        store_columns(
            0,
            [
                mine_g,
                sib_g,
                jnp.where(done_x | done_y, 0.0, 1.0),
                jnp.where(done_x, 1.0, x_g),
                jnp.where(done_y, 1.0, y_g),
            ],
        )

    def column(group, i, start, size):
        return columns[group, pl.ds(start, size), i : i + 1]

    def local_sum(group, start, size):
        where = pl.ds(start, size)
        return (
            column(group, 0, start, size) * mine[group, where].astype(F32)
            + column(group, 1, start, size) * theirs[group, where].astype(F32)
            + column(group, 2, start, size) * shared[group, where]
        )

    def into_sum(total, group):
        def step(i, carry):
            start = pl.multiple_of(i * piece, piece)
            total[pl.ds(start, piece)] = local_sum(group, start, piece)
            return carry

        lax.fori_loop(0, rows // piece, step, 0)

    def merge(group, target_of, recv_of):
        for step in range(steps):
            for first, peer in ((0, nx), (1, ny)):
                start = first * half + step * piece
                merged[group, pl.ds(start, piece)] = local_sum(group, start, piece).astype(BF16)
                link(merged.at[group], target_of(first), start, piece, recv_of(step), peer)

    arrived(gain, sems.at[3])
    norm(0)
    arrived(w_in, sems.at[4])
    arrived(w_down, sems.at[5])
    expert(mine.at[0])
    arrived(s_in, sems.at[6])
    arrived(s_down, sems.at[7])
    common(0)
    serve(0)

    arrived(tally.at[0], meta_recv.at[0])
    arrived(tally.at[0], sems.at[2])
    send(near_routes.at[0], near_routes.at[2], sems.at[2], meta_recv.at[1], {"tp": ny})
    send(near_gates.at[0], near_gates.at[2], sems.at[2], meta_recv.at[1], {"tp": ny})
    token_send(0, half, quarter, 2, 2, nx)
    token_send(0, 0, quarter, 2, 2, ny)
    own_coefficients()
    x_route, y_route = near_routes[0], near_routes[1]
    x_gate, y_gate = near_gates[0], near_gates[1]
    coefficients(1, jnp.where(low, x_route, y_route), jnp.where(low, x_gate, y_gate))
    coefficients(
        2,
        jnp.where(low, y_route, x_route),
        jnp.where(low, y_gate, x_gate),
        relayed=True,
    )

    landed(1, 0, half, 0)
    token_send(1, 0, quarter, 3, 4, ny)
    token_send(1, quarter, quarter, 3, 5, ny)
    lend(1, 0, half)
    landed(1, half, half, 1)
    token_send(1, half, quarter, 3, 4, nx)
    token_send(1, half + quarter, quarter, 3, 5, nx)
    lend(1, half, half)
    token_send(0, half + quarter, quarter, 2, 3, nx)
    token_send(0, quarter, quarter, 2, 3, ny)
    arrived(at_rows(near_routes, 0, 2), meta_recv.at[1])
    d_route = near_routes[2]
    tally[0] = tallied(routes[...]) + tallied(x_route) + tallied(y_route) + tallied(d_route)
    arrived(at_rows(near_routes, 0, 2), sems.at[2])
    tally_send(0, 1, 2, 0, {"tp": sib})
    norm(1)
    expert(mine.at[1])
    arrived(tally.at[1], tally_recv.at[0])
    arrived(tally.at[0], sems.at[2])
    tally[2] = tally[0] + tally[1]
    rounds = list(range(eps))

    @pl.when(above)
    def _():
        pl.semaphore_wait(entered.at[3], 1)

    along_column(rounds[:1])
    serve(1)
    common(1)
    coefficients(3, d_route, near_gates[2])
    arrived(theirs.at[0], result_recv.at[0])
    into_sum(base, 0)
    landed(2, 0, half, 2)
    lend(2, half, quarter)
    lend(2, 0, quarter)
    along_column(rounds[1:2])
    arrived(theirs.at[1], result_recv.at[1])
    merge(1, lambda first: back.at[first], lambda step: back_recv.at[steps])

    landed(3, 0, half, 4)
    lend(3, 0, quarter)
    lend(3, half, quarter)
    landed(3, 0, half, 5)
    lend(3, quarter, quarter)
    lend(3, half + quarter, quarter)
    along_column(rounds[2:3])
    norm(3)
    common(3)
    serve(3)
    expert(mine.at[3])
    landed(2, 0, half, 3)
    lend(2, half + quarter, quarter)
    lend(2, quarter, quarter)
    along_column(rounds[3:])

    @pl.when(column_head)
    def _():
        tally[7] = tally[5] + tally[6] - tally[2]

    hand_on(0)
    arrived(theirs.at[3], result_recv.at[1])
    merge(3, lambda first: passed, lambda step: passed_recv.at[step])
    serve(2)
    norm(2)
    expert(mine.at[2])
    common(2)
    arrived(theirs.at[2], result_recv.at[0])
    into_sum(shared.at[2], 2)
    hand_on(1)
    hand_on(2)

    for step in range(steps):
        arrived(at_rows(passed, 0, 2 * piece), passed_recv.at[step])
        for first, peer in ((1, nx), (0, ny)):
            start = first * half + step * piece
            where = pl.ds(start, piece)
            merged[2, where] = (
                shared[2, where] + column(2, 3, start, piece) * passed[where].astype(F32)
            ).astype(BF16)
            link(merged.at[2], back.at[1 - first], start, piece, back_recv.at[step], peer)

    arrived(at_rows(back.at[0], 0, rows), back_recv.at[steps])

    def early(i, carry):
        for first in range(2):
            start = pl.multiple_of(first * half + i * piece, piece)
            where = pl.ds(start, piece)
            base[where] = base[where] + column(0, 3 + first, start, piece) * back[
                first, where
            ].astype(F32)
        return carry

    lax.fori_loop(0, steps, early, 0)

    hand_on(3)
    hand_on(4)
    counts = lax.dot_general(
        jnp.ones((8, rows), F32),
        tally[7],
        (((1,), (1,)), ((), ())),
        precision=lax.Precision.HIGHEST,
        preferred_element_type=F32,
    )
    load[...] = counts[0:1, :] * (n / (rows * 2 * n * eps))

    for step in range(steps):
        arrived(at_rows(back.at[0], 0, 2 * piece), back_recv.at[step])
        for first in range(2):
            start = (1 - first) * half + step * piece
            where = pl.ds(start, piece)
            out[where] = (
                base[where] + column(0, 3 + first, start, piece) * back[first, where].astype(F32)
            ).astype(BF16)

    arrived(at_rows(blocks, 0, 6), sems.at[0])
    arrived(blocks, sems.at[1])
    for number, test in ((3, above), (4, below)):

        @pl.when(test)
        def _():
            arrived(tally.at[0], sems.at[number])

    for test, peers in handers[:-1]:

        @pl.when(test)
        def _():
            arrived(at_rows(tally, 0, len(peers)), sems.at[2])


def write_out(mixed, load, mixed_out, load_out, sem):
    copies = [
        pltpu.make_async_copy(mixed, mixed_out, sem.at[0]),
        pltpu.make_async_copy(load, load_out, sem.at[1]),
    ]
    for copy in copies:
        copy.start()
    for copy in copies:
        copy.wait()


def per_device(
    tokens,
    norm_gain,
    routes,
    gates,
    expert_gate,
    expert_up,
    expert_down,
    shared_gate,
    shared_up,
    shared_down,
):
    n, eps = lax.axis_size("tp"), lax.axis_size("ep")
    rows, width = tokens.shape
    top = routes.shape[1]
    cap = 2 * rows * top // n
    units = expert_gate.shape[2]
    vmem = pl.BlockSpec(memory_space=pltpu.VMEM)
    hbm = pl.BlockSpec(memory_space=pl.ANY)
    dma = pltpu.SemaphoreType.DMA
    if n == 8 and top == 2:
        body = functools.partial(square, eps)
        small = hbm
        scratch = [
            pltpu.VMEM((8, rows, width), BF16),
            pltpu.VMEM((top, rows), jnp.int32),
            pltpu.VMEM((top, rows), F32),
            pltpu.VMEM((1, width), F32),
            pltpu.VMEM((3, top, rows), jnp.int32),
            pltpu.VMEM((3, top, rows), F32),
            pltpu.VMEM((8, n, rows), F32),
            pltpu.VMEM((4, 8, rows), F32),
            pltpu.VMEM((4, rows, 8), F32),
            pltpu.VMEM((2, rows, width), BF16),
            pltpu.VMEM((rows, units), BF16),
            pltpu.VMEM((4, rows, width), BF16),
            pltpu.VMEM((4, rows, width), BF16),
            pltpu.VMEM((4, rows, width), BF16),
            pltpu.VMEM((4, rows, width), F32),
            pltpu.VMEM((4, rows, width), BF16),
            pltpu.VMEM((rows, width), BF16),
            pltpu.VMEM((2, rows, width), BF16),
            pltpu.VMEM((rows, width), F32),
            pltpu.VMEM((2, *expert_gate.shape[1:]), BF16),
            pltpu.VMEM(expert_down.shape[1:], BF16),
            pltpu.VMEM((2, *shared_gate.shape), BF16),
            pltpu.VMEM(shared_down.shape, BF16),
            dma((8,)),
            pltpu.SemaphoreType.REGULAR((4,)),
            dma((2,)),
            dma((4,)),
            dma((6,)),
            dma((2,)),
            dma((2,)),
            dma((rows // 32,)),
            dma((rows // 32 + 1,)),
        ]
    else:
        body = functools.partial(direct, n, eps, cap)
        small = vmem
        scratch = [
            pltpu.VMEM((rows, width), BF16),
            pltpu.VMEM((n, rows, width), BF16),
            pltpu.VMEM((n, top, rows), jnp.int32),
            pltpu.VMEM((eps, n, top, rows), jnp.int32),
            pltpu.VMEM((rows, width), BF16),
            pltpu.VMEM((rows, units), BF16),
            pltpu.VMEM((n, cap, width), BF16),
            pltpu.VMEM((n, cap, width), BF16),
            pltpu.VMEM((rows, width), F32),
            pltpu.VMEM(expert_gate.shape[1:], BF16),
            pltpu.VMEM(expert_up.shape[1:], BF16),
            pltpu.VMEM(expert_down.shape[1:], BF16),
            pltpu.VMEM(shared_gate.shape, BF16),
            pltpu.VMEM(shared_up.shape, BF16),
            pltpu.VMEM(shared_down.shape, BF16),
            dma((6,)),
            dma((2,)),
            dma((n - 1,)),
            dma((n,)),
            dma((max(1, eps - 1),)),
            dma((eps,)),
            dma((2 * (n - 1),)),
            dma((n, 2)),
            dma((n,)),
            dma((n,)),
        ]
    mixed, load = pl.pallas_call(
        body,
        out_shape=(
            pltpu.VMEM((rows, width), BF16),
            pltpu.VMEM((1, n), F32),
        ),
        in_specs=[hbm] + [small] * 3 + [hbm] * 6,
        out_specs=(vmem, vmem),
        scratch_shapes=scratch,
        compiler_params=pltpu.CompilerParams(
            collective_id=0, has_side_effects=True
        ),
    )(
        tokens,
        routes.T,
        gates.T,
        norm_gain.reshape(1, width),
        expert_gate,
        expert_up,
        expert_down,
        shared_gate,
        shared_up,
        shared_down,
    )
    mixed, load = pl.pallas_call(
        write_out,
        out_shape=(
            jax.ShapeDtypeStruct((rows, width), BF16),
            jax.ShapeDtypeStruct((1, n), F32),
        ),
        in_specs=[vmem] * 2,
        out_specs=(hbm, hbm),
        scratch_shapes=[dma((2,))],
        compiler_params=pltpu.CompilerParams(vmem_limit_bytes=1 << 20),
    )(mixed, load)
    return mixed, load.reshape(n)


def solution(mesh):
    placed = (
        P(("ep", "tp"), None),
        P(),
        P(("ep", "tp"), None),
        P(("ep", "tp"), None),
        P("tp", None, None),
        P("tp", None, None),
        P("tp", None, None),
        P(),
        P(),
        P(),
    )
    return jax.shard_map(
        per_device,
        mesh=mesh,
        in_specs=placed,
        out_specs=(P(("ep", "tp"), None), P()),
        check_vma=False,
    )
```
